32 devices in a mesh: ep: 8 (over z, x), tp: 4 (over y, core).
Axes of the slice: x: 2, y: 2, z: 4, core: 2. Of those that a mesh axis runs over, the one named last changes fastest.
Arguments:
- queries: bfloat16 [4096, 1024], P('ep', 'tp'), may hold values from -6 to 6
- forget_forward_logits: bfloat16 [4096, 1024], P('ep', 'tp'), may hold values from -6 to 12
- forget_backward_logits: bfloat16 [4096, 1024], P('ep', 'tp'), may hold values from -6 to 12
- values: bfloat16 [4096, 1024], P('ep', 'tp'), may hold values from -6 to 6
- output_gate_logits: bfloat16 [4096, 1024], P('ep', 'tp'), may hold values from -6 to 6
- lower_bound_forward: float32 [1024], P('tp')
- lower_bound_backward: float32 [1024], P('tp')
- extra_log_decay: float32 [4096, 8], P('ep', 'tp'), may hold values from -2 to 0
- head_norm_scale: float32 [1024], P('tp'), may hold values from 0.1 to 1.9
- output_projection: bfloat16 [1024, 2048], P('tp'), may hold values from -0.1875 to 0.1875
- second_residual: bfloat16 [4096, 2048], P('ep'), may hold values from -6 to 6
- expert_norm_scale: float32 [2048], replicated, may hold values from 0.1 to 1.9
- routes: int32 [4096, 2], P('ep'), may hold values from 0 to 7, all different within a row; in each aligned block of 128 rows (0 to 127, 128 to 255, ...) at most 64 rows name the same one
- specialist_mixing_factor: float32 [4096, 2], P(('ep', 'tp')), may hold values from 0.1 to 1
- expert_gate_matrix: bfloat16 [8, 2048, 1024], P('ep', None, 'tp'), may hold values from -0.125 to 0.125
- expert_up_matrix: bfloat16 [8, 2048, 1024], P('ep', None, 'tp'), may hold values from -0.125 to 0.125
- expert_down_matrix: bfloat16 [8, 1024, 2048], P('ep', 'tp'), may hold values from -0.1875 to 0.1875
Outputs:
- mixer_output: bfloat16 [4096, 2048], P(('ep', 'tp'))
- routed_output: bfloat16 [4096, 2048], P(('ep', 'tp'))
The draws below stay inside these ranges and needn't reach their ends.
Inputs may be any that keep to these rules, and one draw needn't show every extreme that they name: `routes`: in each aligned block of 128 rows no expert is named by more than 64 rows; the 2 experts of a row differ.
All inputs are finite; a program needn't handle non-finite values.
Results may differ from the reference program's by a relative error of at most 0.014.
Values may be sent and summed in bfloat16 or wider, within the bound.
No kernel may reach another device: no remote copies, remote signals or barrier semaphores. Data moves between devices by JAX's collectives and lax.ppermute only.
A program may use at most 128 MiB of HBM per device.

```python
import math
import jax
import jax.numpy as jnp
import numpy as np
from jax import lax

D = 2048
RECURRENT_HEADS = 8
DK = 128
DV = 128
FF = 1024
TOPK = 2
SPAN = 64
ROWS = 128
KEY_WIDTH = 1024
VAL_WIDTH = 1024
GROUP_WIDTH = 256
EXPERT_PART = 256
EXPERTS = 8
CAPQ = 64
TOKENS_A = 4096
TOKENS_B = 4096
N_EP = 8
N_TP = 4


def floor_common(key, salt):
    key = jax.random.fold_in(key, salt)
    key_order, key_slow, key_fast = jax.random.split(key, 3)
    ordering = jax.random.permutation(key_order, RECURRENT_HEADS)
    slow_heads = ordering < RECURRENT_HEADS // 2
    slow_rate = jax.random.uniform(key_slow, (RECURRENT_HEADS, DK), jnp.float32, 0.3, 2.0) / TOKENS_A
    fast_rate = jnp.exp(jax.random.uniform(key_fast, (RECURRENT_HEADS, DK), jnp.float32, math.log(0.025), math.log(0.1)))
    decay_rate = jnp.where(slow_heads[:, None], slow_rate, fast_rate)
    return (jnp.log1p(-decay_rate) - jnp.log(decay_rate)).reshape(RECURRENT_HEADS * DK).astype(jnp.float32)


def draw_lower_bound_forward(key, part):
    return floor_common(key, 11)


def draw_lower_bound_backward(key, part):
    return floor_common(key, 12)


def forget_common(key, salt):
    key = jax.random.fold_in(key, salt)
    key_base, key_run = jax.random.split(key, 2)
    base = jnp.clip(1.5 * jax.random.normal(key_base, (TOKENS_A, RECURRENT_HEADS, DK), jnp.float32), -6.0, 6.0)
    run_length = 4 * SPAN
    run_count = (TOKENS_A + run_length - 1) // run_length
    lifted = 6.0 * jax.random.randint(key_run, (run_count, RECURRENT_HEADS), 0, 2).astype(jnp.float32)
    position_block = jnp.arange(TOKENS_A, dtype=jnp.int32) // run_length
    offsets = lifted[position_block]
    return (base + offsets[:, :, None]).reshape(TOKENS_A, RECURRENT_HEADS * DK).astype(jnp.float32)


def draw_forget_forward_logits(key, part):
    return forget_common(key, 21).astype(jnp.bfloat16)


def draw_forget_backward_logits(key, part):
    return forget_common(key, 22).astype(jnp.bfloat16)


def draw_extra_log_decay(key, part):
    key_rate, key_place, key_depth = jax.random.split(key, 3)
    span_rows = TOKENS_A // EXPERTS
    factor = jnp.exp(jax.random.uniform(key_rate, (EXPERTS, RECURRENT_HEADS), jnp.float32, 0.0, math.log(3.0)))
    token_position = jnp.arange(TOKENS_A, dtype=jnp.int32)
    owner_block = token_position // span_rows
    stable_state = -0.2 / TOKENS_A * factor[owner_block]
    slot_positions = jax.random.randint(key_place, (2, RECURRENT_HEADS), 0, TOKENS_A)
    cumulative_decay = jnp.log(jax.random.uniform(key_depth, (2, RECURRENT_HEADS), jnp.float32, 0.55, 0.8))
    extra_decay_hits = token_position[:, None, None] == slot_positions[None, :, :]
    return (stable_state + jnp.sum(jnp.where(extra_decay_hits, cumulative_decay[None], 0.0), axis=1)).astype(jnp.float32)


def shard_levels(key, shape, cuts, low, high):
    level, own = 1.0, jax.random.fold_in(key, 6)
    for position, shards_of in cuts:
        draws = jnp.exp(jax.random.uniform(jax.random.fold_in(own, position), (shards_of,), jnp.float32, low / len(cuts), high / len(cuts)))
        level = level * jnp.repeat(draws, shape[position] // shards_of).reshape([-1 if axis == position else 1 for axis in range(len(shape))])
    return level


def deal_out(own_key, own, number, rows, count, top, most, lean):
    ranking = jax.random.permutation(own_key, count)
    crowded, common = load_shares(count, rows * top, most, lean, True), load_shares(count, rows * top, most, lean, False)
    places = jnp.arange(count)

    def named(sizes, offset_by):
        used = int((sizes > 0).sum())
        fixed = max(1, used // 4)
        passed = fixed + (places - fixed + offset_by * (used - fixed)) % max(1, count - fixed)
        return jnp.zeros((count,), jnp.int32).at[ranking[jnp.where(places < fixed, places, passed)]].set(jnp.asarray(sizes, jnp.int32))

    sizes = jnp.where(number % 4 == 0, named(crowded, number // 4), named(common, number - number // 4 - 1))
    mixed = jax.random.permutation(jax.random.fold_in(own, 3), count)
    source_of, receiver = mixed[0:count // 2 * 2:2], mixed[1:count // 2 * 2:2]
    slack = jnp.minimum(sizes[source_of] - 1, most - sizes[receiver]) // 2
    slack = jnp.where((source_of == ranking[0]) | (receiver == ranking[0]) | (sizes[receiver] == 0), 0, jnp.maximum(slack, 0))
    passed = jax.random.randint(jax.random.fold_in(own, 4), (count // 2,), 0, 1 << 20) % (slack + 1)
    sizes = sizes.at[source_of].add(-passed).at[receiver].add(passed)
    members = jnp.searchsorted(jnp.cumsum(sizes), jnp.arange(rows * top), side="right").astype(jnp.int32)
    table = members.reshape(top, rows).T
    table = table[jax.random.permutation(jax.random.fold_in(own, 1), rows)]
    offset_by = jax.random.randint(jax.random.fold_in(own, 2), (rows, 1), 0, top)
    return jnp.take_along_axis(table, (jnp.arange(top)[None, :] + offset_by) % top, axis=1)


def load_shares(count, total, bound, skew, full):
    weights = [(1 << 20) // math.isqrt(standing ** skew) + 1 for standing in range(1, count + 1)]
    largest = bound if full else min(bound, max(-(-total // count), total * weights[0] // sum(weights)))
    least = 1 if total - largest >= count - 1 else 0
    given, rest = [largest] + [least] * (count - 1), total - largest - least * (count - 1)
    while rest > 0:
        movable = [i for i in range(1, count) if given[i] < largest] or [i for i in range(1, count) if given[i] < bound]
        mass, remaining = sum([weights[i] for i in movable]), rest
        for i in movable:
            extra = min(bound - given[i], max(1, remaining * weights[i] // mass), rest)
            given[i] = given[i] + extra
            rest = rest - extra
    return np.array(given)


def noise(stream_key, shape, deviation, bound, shards=(), held_as=jnp.bfloat16):
    loudness = shard_levels(stream_key, shape, shards, -0.22, 0.18) if shards else 1.0
    entries = jax.random.normal(stream_key, shape, jnp.float32) * deviation * loudness
    return jnp.minimum(jnp.maximum(entries, -bound), bound).astype(held_as)


def setup_inputs(seed: int = 0) -> dict:
    arg_keys = jax.random.split(jax.random.key(seed), 18)
    queries = noise(arg_keys[0], (TOKENS_A, KEY_WIDTH), 1.0, 6.0, ((0, 8), (1, 4)))
    forget_forward_logits = draw_forget_forward_logits(jax.random.fold_in(arg_keys[17], 71), 0)
    forget_backward_logits = draw_forget_backward_logits(jax.random.fold_in(arg_keys[17], 71), 0)
    values = noise(arg_keys[3], (TOKENS_A, VAL_WIDTH), 1.0, 6.0, ((0, 8), (1, 4)))
    output_gate_logits = noise(arg_keys[4], (TOKENS_A, VAL_WIDTH), 1.0, 6.0, ((0, 8), (1, 4)))
    lower_bound_forward = draw_lower_bound_forward(jax.random.fold_in(arg_keys[17], 71), 0)
    lower_bound_backward = draw_lower_bound_backward(jax.random.fold_in(arg_keys[17], 71), 0)
    extra_log_decay = draw_extra_log_decay(jax.random.fold_in(arg_keys[17], 71), 0)
    head_norm_scale = jnp.clip(1.0 + 0.18 * jax.random.normal(arg_keys[8], (VAL_WIDTH,), jnp.float32), 0.1, 1.9)
    output_projection = noise(arg_keys[9], (VAL_WIDTH, D), VAL_WIDTH ** -0.5, 0.1875, ((0, 4),))
    second_residual = noise(arg_keys[10], (TOKENS_B, D), 1.0, 6.0, ((0, 8),))
    expert_norm_scale = jnp.clip(1.0 + 0.18 * jax.random.normal(arg_keys[11], (D,), jnp.float32), 0.1, 1.9)
    routes_keys = jax.random.split(jax.random.fold_in(arg_keys[12], 1), TOKENS_B // ROWS)
    routes_turns = jax.random.permutation(jax.random.fold_in(arg_keys[12], 3), TOKENS_B // ROWS)
    routes = jax.vmap(lambda own, number: deal_out(jax.random.fold_in(arg_keys[12], 2), own, number, ROWS, EXPERTS, TOPK, CAPQ, 2))(routes_keys, routes_turns).reshape((TOKENS_B, TOPK))
    specialist_mixing_factor = jnp.clip(0.1 + 0.9 * jax.random.uniform(arg_keys[13], (TOKENS_B, TOPK), jnp.float32) ** shard_levels(arg_keys[13], (TOKENS_B, TOPK), ((0, 32),), -0.2, 0.2), 0.1, 1.0)
    expert_gate_matrix = noise(arg_keys[14], (EXPERTS, D, FF), D ** -0.5, 0.125, ((0, 8), (2, 4)))
    expert_up_matrix = noise(arg_keys[15], (EXPERTS, D, FF), D ** -0.5, 0.125, ((0, 8), (2, 4)))
    expert_down_matrix = noise(arg_keys[16], (EXPERTS, FF, D), FF ** -0.5, 0.1875, ((0, 8), (1, 4)))
    return dict(queries=queries, forget_forward_logits=forget_forward_logits, forget_backward_logits=forget_backward_logits, values=values, output_gate_logits=output_gate_logits, lower_bound_forward=lower_bound_forward, lower_bound_backward=lower_bound_backward, extra_log_decay=extra_log_decay, head_norm_scale=head_norm_scale, output_projection=output_projection, second_residual=second_residual, expert_norm_scale=expert_norm_scale, routes=routes, specialist_mixing_factor=specialist_mixing_factor, expert_gate_matrix=expert_gate_matrix, expert_up_matrix=expert_up_matrix, expert_down_matrix=expert_down_matrix)


EPS = 1e-06
PRECISE_PRODUCT = lax.Precision.HIGHEST

def block_pass(feature, key_matrix_rows, value_rows, log_forget_decay):
    row_count, number_of_heads, channels = feature.shape
    blocks = row_count // SPAN
    lower_mask = jnp.tril(jnp.ones((SPAN, SPAN), bool))[:, :, None, None]

    def shaped(tensor):
        return tensor.reshape(blocks, SPAN, number_of_heads, tensor.shape[-1])

    def advance(progress, inputs):
        recurrent_memory, offset = progress
        query_tile_rows, address_piece_entries, content_piece_entries, decay_block = inputs
        progressive_summary = jnp.cumsum(decay_block, axis=0)
        spread_log = jnp.where(lower_mask, progressive_summary[:, None] - progressive_summary[None, :], -jnp.inf)
        scores = lax.optimization_barrier(jnp.sum(query_tile_rows[:, None] * address_piece_entries[None, :] * jnp.exp(spread_log), axis=-1))
        inner_part = jnp.einsum('tsh,shv->thv', scores, content_piece_entries, precision=PRECISE_PRODUCT)
        handed_summary = jnp.einsum('wbf,bfl->wbl', query_tile_rows * jnp.exp(progressive_summary), recurrent_memory, precision=PRECISE_PRODUCT)
        segment_fading_total = progressive_summary[-1]
        trained_portion = jnp.einsum('gkf,gkr->kfr', address_piece_entries * jnp.exp(segment_fading_total[None] - progressive_summary), content_piece_entries, precision=PRECISE_PRODUCT)
        recurrent_memory = jnp.exp(segment_fading_total)[:, :, None] * recurrent_memory + trained_portion
        return ((recurrent_memory, offset + segment_fading_total), (inner_part + handed_summary, query_tile_rows * jnp.exp(progressive_summary + offset)))
    initial = (jnp.zeros((number_of_heads, channels, value_rows.shape[-1]), jnp.float32), jnp.zeros((number_of_heads, channels), jnp.float32))
    (recurrent_memory, decay_total), (output_rows, query_decay_reach) = lax.scan(advance, initial, (shaped(feature), shaped(key_matrix_rows), shaped(value_rows), shaped(log_forget_decay)))
    return (output_rows.reshape(row_count, number_of_heads, -1), query_decay_reach.reshape(row_count, number_of_heads, channels), recurrent_memory, decay_total)

def forget_gate_terms(forget_gate_input, lower_bound_logit, extra_decay_rows, number_of_heads):
    row_count = forget_gate_input.shape[0]
    widened_values = forget_gate_input.astype(jnp.float32).reshape(row_count, number_of_heads, -1)
    lower_bound_share = jax.nn.sigmoid(lower_bound_logit).reshape(number_of_heads, -1)
    remaining_fraction = jax.nn.sigmoid(-lower_bound_logit).reshape(number_of_heads, -1)
    log_forget_decay = jnp.log(lower_bound_share + remaining_fraction * jax.nn.sigmoid(widened_values)) + extra_decay_rows[:, :, None]
    return (remaining_fraction * jax.nn.sigmoid(-widened_values), log_forget_decay)

def finish_heads(combined, head_norm_scale, output_gate_logits, number_of_heads):
    mean_square = lax.optimization_barrier(jnp.mean(combined * combined, axis=-1, keepdims=True))
    scaled = combined * lax.rsqrt(mean_square + EPS) * head_norm_scale.reshape(number_of_heads, -1)
    opened = scaled * jax.nn.silu(output_gate_logits.astype(jnp.float32)).reshape(combined.shape)
    return opened.astype(jnp.bfloat16).reshape(combined.shape[0], -1)

def normalize(tensor, gain):
    widened_values = tensor.astype(jnp.float32)
    return (widened_values * lax.rsqrt(lax.optimization_barrier(jnp.mean(widened_values * widened_values, axis=-1, keepdims=True)) + EPS) * gain).astype(jnp.bfloat16)

def reference(queries, forget_forward_logits, forget_backward_logits, values, output_gate_logits, lower_bound_forward, lower_bound_backward, extra_log_decay, head_norm_scale, output_projection, second_residual, expert_norm_scale, routes, specialist_mixing_factor, expert_gate_matrix, expert_up_matrix, expert_down_matrix):
    feature = jax.nn.silu(queries.astype(jnp.float32)).reshape(TOKENS_A, RECURRENT_HEADS, DK)
    value_rows = values.astype(jnp.float32).reshape(TOKENS_A, RECURRENT_HEADS, DV)
    combined = jnp.zeros(value_rows.shape, jnp.float32)
    for forget_gate_input, lower_bound_logit, reverse in ((forget_forward_logits, lower_bound_forward, False), (forget_backward_logits, lower_bound_backward, True)):
        key_matrix_rows, log_forget_decay = forget_gate_terms(forget_gate_input, lower_bound_logit, extra_log_decay, RECURRENT_HEADS)
        if reverse:
            output_rows = block_pass(jnp.flip(feature, 0), jnp.flip(key_matrix_rows, 0), jnp.flip(value_rows, 0), jnp.flip(log_forget_decay, 0))[0]
            output_rows = jnp.flip(output_rows, 0)
        else:
            output_rows = block_pass(feature, key_matrix_rows, value_rows, log_forget_decay)[0]
        combined = combined + output_rows
    mixer_hidden = finish_heads(combined, head_norm_scale, output_gate_logits, RECURRENT_HEADS)
    summed = jnp.zeros((TOKENS_A, D), jnp.float32)
    for group_index in range(N_TP):
        lower_edge = group_index * GROUP_WIDTH
        partial_value = jnp.dot(mixer_hidden[:, lower_edge:lower_edge + GROUP_WIDTH], output_projection[lower_edge:lower_edge + GROUP_WIDTH], preferred_element_type=jnp.float32)
        summed = summed + lax.optimization_barrier(partial_value.astype(jnp.bfloat16)).astype(jnp.float32)
    mixer_output = summed.astype(jnp.bfloat16)
    routed_normed = normalize(second_residual, expert_norm_scale)
    slot_total = N_EP * N_TP * CAPQ
    token_ids = jnp.arange(TOKENS_B, dtype=jnp.int32)

    def one_expert(accumulated, expert):
        chosen = routes == expert
        weight = lax.optimization_barrier(jnp.sum(jnp.where(chosen, specialist_mixing_factor, 0.0), axis=1))
        member = jnp.any(chosen, axis=1)
        token_position = (jnp.cumsum(member.astype(jnp.int32)) - 1).astype(jnp.int32)
        token_position = jnp.where(member, token_position, slot_total).astype(jnp.int32)
        slot_table = jnp.zeros((slot_total + 1,), jnp.int32).at[token_position].set(token_ids)[:slot_total]
        slot_weight = jnp.zeros((slot_total + 1,), jnp.float32).at[token_position].set(weight)[:slot_total]
        picked = routed_normed[slot_table]
        gated = jnp.dot(picked, expert_gate_matrix[expert], preferred_element_type=jnp.float32)
        lifted = jnp.dot(picked, expert_up_matrix[expert], preferred_element_type=jnp.float32)
        expert_hidden = (jax.nn.silu(gated) * lifted).astype(jnp.bfloat16)
        down_rows = expert_down_matrix[expert]
        result = jnp.zeros((slot_total, D), jnp.float32)
        for group_index in range(N_TP):
            lower_edge = group_index * EXPERT_PART
            partial_value = jnp.dot(expert_hidden[:, lower_edge:lower_edge + EXPERT_PART], down_rows[lower_edge:lower_edge + EXPERT_PART], preferred_element_type=jnp.float32)
            result = result + lax.optimization_barrier(partial_value.astype(jnp.bfloat16)).astype(jnp.float32)
        expert_result = lax.optimization_barrier(result.astype(jnp.bfloat16)).astype(jnp.float32)
        accumulated = accumulated.at[slot_table].add(slot_weight[:, None] * expert_result)
        return (accumulated, None)
    accumulated = lax.scan(one_expert, jnp.zeros((TOKENS_B, D), jnp.float32), jnp.arange(EXPERTS, dtype=jnp.int32))[0]
    routed_output = accumulated.astype(jnp.bfloat16)
    return (mixer_output, routed_output)
```

```python
import functools
import jax
import jax.numpy as jnp
from jax import lax
from jax.experimental import pallas as pl
from jax.experimental.pallas import tpu as pltpu
from jax.sharding import PartitionSpec as P

TOPK = 2
EPS = 1e-06
CHUNK = 128
FINE = 16
DIRECT_EP = 8
DOWN_PARTS = 2
F32 = jnp.float32
BF16 = jnp.bfloat16

NT = (((1,), (1,)), ((), ()))
TN = (((0,), (0,)), ((), ()))
VM = pl.BlockSpec(memory_space=pltpu.VMEM)
SM = pl.BlockSpec(memory_space=pltpu.SMEM)
HBM = pl.BlockSpec(memory_space=pl.ANY)


def cost(flops, moved, exps=0):
    return pl.CostEstimate(flops=int(flops), bytes_accessed=int(moved), transcendentals=int(exps))


def params():
    return pltpu.CompilerParams(vmem_limit_bytes=56 * 1024 * 1024)


def dot(a, b, dims=(((1,), (0,)), ((), ()))):
    return lax.dot_general(a, b, dims, preferred_element_type=F32)


def gate_terms(logits, bound, extra):
    wide = logits.astype(F32)
    grown = jnp.exp(-wide)
    opened = 1.0 / (1.0 + grown)
    floor = jax.nn.sigmoid(bound)
    rest = jax.nn.sigmoid(-bound)
    return rest * (grown * opened), jnp.log(floor + rest * opened) + extra


def running_sum(decay, lower):
    rows, width = decay.shape
    high = decay.astype(BF16)
    low = (decay - high.astype(F32)).astype(BF16)
    carry = jnp.zeros((1, width), F32)
    pieces = []
    for start in range(0, rows, CHUNK):
        both = dot(
            lower,
            jnp.concatenate([high[start : start + CHUNK], low[start : start + CHUNK]], axis=1),
        )
        piece = both[:, :width] + both[:, width:] + carry
        carry = piece[CHUNK - 1 : CHUNK]
        pieces.append(piece)
    return jnp.concatenate(pieces, axis=0)


def recurrence_kernel(
    ep, heads, direct, me_ref, q_ref, ff_ref, fb_ref, v_ref, lf_ref, lb_ref, extra_ref, *refs
):
    out_ref, reach_f_ref, reach_b_ref = refs[:3]
    message_refs = refs[3:-3]
    mix_ref, msg_f, msg_b = refs[-3:]
    rows = q_ref.shape[0]
    width = q_ref.shape[1] // heads
    tail = 16
    row = lax.broadcasted_iota(jnp.int32, (CHUNK, CHUNK), 0)
    col = lax.broadcasted_iota(jnp.int32, (CHUNK, CHUNK), 1)
    lower = jnp.where(row >= col, 1.0, 0.0).astype(BF16)
    tail_row = lax.broadcasted_iota(jnp.int32, (tail, width), 0)
    decays = [jnp.zeros((tail, width), F32), jnp.zeros((tail, width), F32)]
    for head in range(heads):
        lanes = slice(head * width, (head + 1) * width)
        q = q_ref[:, lanes].astype(F32)
        q = q / (1.0 + jnp.exp(-q))
        v = v_ref[:, lanes]
        extra = extra_ref[:, head : head + 1]
        kf, gf = gate_terms(ff_ref[:, lanes], lf_ref[:, lanes], extra)
        kb, gb = gate_terms(fb_ref[:, lanes], lb_ref[:, lanes], extra)
        b = running_sum(gf, lower)
        total_f = b[rows - 1 : rows]
        ahead = running_sum(gb, lower)
        total_b = ahead[rows - 1 : rows]
        c = total_b - ahead + gb

        half = rows // 2
        while half >= CHUNK:
            for first in range(0, rows, 2 * half):
                mid, last = first + half, first + 2 * half
                one, two = slice(first, mid), slice(mid, last)
                ref_f, ref_b = b[mid - 1 : mid], c[mid : mid + 1]
                mix_ref[two, one] = dot(
                    (q[two] * jnp.exp(b[two] - ref_f)).astype(BF16),
                    (kf[one] * jnp.exp(ref_f - b[one])).astype(BF16),
                    NT,
                ).astype(BF16)
                mix_ref[one, two] = dot(
                    (q[one] * jnp.exp(c[one] - ref_b)).astype(BF16),
                    (kb[two] * jnp.exp(ref_b - c[two])).astype(BF16),
                    NT,
                ).astype(BF16)
            half //= 2
        for start in range(0, rows, CHUNK):
            here = slice(start, start + CHUNK)
            qc, kfc, kbc, bc, cc = q[here], kf[here], kb[here], b[here], c[here]
            mid_f, mid_b = [], []
            for first in range(0, CHUNK, FINE):
                at = first + FINE // 2
                mid_f.append(jnp.broadcast_to(bc[at - 1 : at], (FINE, width)))
                mid_b.append(jnp.broadcast_to(cc[at : at + 1], (FINE, width)))
            df = bc - jnp.concatenate(mid_f, axis=0)
            db = cc - jnp.concatenate(mid_b, axis=0)
            near_f = dot((qc * jnp.exp(df)).astype(BF16), (kfc * jnp.exp(-df)).astype(BF16), NT)
            near_b = dot((qc * jnp.exp(db)).astype(BF16), (kbc * jnp.exp(-db)).astype(BF16), NT)
            scores = jnp.where(row >= col, near_f, 0.0) + jnp.where(row <= col, near_b, 0.0)
            half = FINE
            while half < CHUNK:
                q_side, k_side = [], []
                for first in range(0, CHUNK, 2 * half):
                    mid, last = first + half, first + 2 * half
                    one, two = slice(first, mid), slice(mid, last)
                    ref_f, ref_b = bc[mid - 1 : mid], cc[mid : mid + 1]
                    q_side.append(qc[one] * jnp.exp(cc[one] - ref_b))
                    q_side.append(qc[two] * jnp.exp(bc[two] - ref_f))
                    k_side.append(kfc[one] * jnp.exp(ref_f - bc[one]))
                    k_side.append(kbc[two] * jnp.exp(ref_b - cc[two]))
                far = dot(
                    jnp.concatenate(q_side, axis=0).astype(BF16),
                    jnp.concatenate(k_side, axis=0).astype(BF16),
                    NT,
                )
                scores = jnp.where(row // half == col // half, scores, far)
                half *= 2
            mix_ref[here, here] = scores.astype(BF16)
        out_ref[:, lanes] = dot(mix_ref[...], v)
        reach_f_ref[:, lanes] = (q * jnp.exp(b)).astype(BF16)
        reach_b_ref[:, lanes] = (q * jnp.exp(c)).astype(BF16)
        for which, message, key, run, total in (
            (0, msg_f, kf, b, total_f),
            (1, msg_b, kb, c, total_b),
        ):
            state = dot(v, (key * jnp.exp(total - run)).astype(BF16), TN)
            message[lanes, :] = state.astype(BF16)
            high = total.astype(BF16).astype(F32)
            decays[which] = jnp.where(tail_row == head, high, decays[which])
            decays[which] = jnp.where(tail_row == heads + head, total - high, decays[which])
    edge = heads * width
    msg_f[edge : edge + tail, :] = decays[0].astype(BF16)
    msg_b[edge : edge + tail, :] = decays[1].astype(BF16)
    me = me_ref[0]
    for step in range(1, ep):
        if direct:
            later = me + step < ep
            target = message_refs[step - 1]

            @pl.when(later)
            def _(target=target):
                target[...] = msg_f[...]

            @pl.when(jnp.logical_not(later))
            def _(target=target):
                target[...] = msg_b[...]
    if not direct:

        def fill(place, carry):
            message_refs[0][place] = jnp.where(place > me, msg_f[...], msg_b[...])
            return carry

        lax.fori_loop(0, ep, fill, 0)


def finish_kernel(
    ep, tp, heads, direct, me_ref, out_ref, reach_f_ref, reach_b_ref, gate_ref, gain_ref, w_ref, *refs
):
    count = ep - 1 if direct else 1
    arrived = refs[:count]
    pieces = refs[count : count + tp]
    hidden_ref, in_f, in_b = refs[count + tp :]
    rows = out_ref.shape[0]
    width = out_ref.shape[1] // heads
    edge = heads * width
    me, quarter = me_ref[0], me_ref[1]
    in_f[...] = jnp.zeros_like(in_f)
    in_b[...] = jnp.zeros_like(in_b)

    def join(state_ref, read):
        decay = read(slice(edge, edge + 16)).astype(F32)
        for head in range(heads):
            lanes = slice(head * width, (head + 1) * width)
            total = decay[head : head + 1] + decay[heads + head : heads + head + 1]
            state_ref[lanes, :] = state_ref[lanes, :] * jnp.exp(total) + read(lanes).astype(F32)

    if direct:
        for step in range(ep - 1, 0, -1):

            @pl.when(step <= me)
            def _(step=step):
                join(in_f, lambda part: arrived[step - 1][part, :])

        for step in range(1, ep):

            @pl.when(step > me)
            def _(step=step):
                join(in_b, lambda part: arrived[step - 1][part, :])

    else:

        def forward(place, carry):
            join(in_f, lambda part: arrived[0][place, part, :])
            return carry

        def backward(place, carry):
            join(in_b, lambda part: arrived[0][ep - 1 - place, part, :])
            return carry

        lax.fori_loop(0, me, forward, 0)
        lax.fori_loop(0, ep - 1 - me, backward, 0)
    for head in range(heads):
        lanes = slice(head * width, (head + 1) * width)
        combined = (
            out_ref[:, lanes]
            + dot(reach_f_ref[:, lanes], in_f[lanes, :].astype(BF16), NT)
            + dot(reach_b_ref[:, lanes], in_b[lanes, :].astype(BF16), NT)
        )
        square = jnp.mean(combined * combined, axis=-1, keepdims=True)
        gate = gate_ref[:, lanes].astype(F32)
        gate = gate / (1.0 + jnp.exp(-gate))
        scaled = combined * lax.rsqrt(square + EPS) * gain_ref[:, lanes]
        hidden_ref[:, lanes] = (scaled * gate).astype(BF16)
    block = rows // tp
    for piece in range(tp):
        start = pl.multiple_of((quarter ^ piece) * block, block)
        part = hidden_ref[pl.ds(start, block), :]
        pieces[piece][...] = dot(part, w_ref[...]).astype(BF16)


def swap(array, axis, bit):
    size = lax.axis_size(axis)
    return lax.ppermute(array, axis, [(place, place ^ bit) for place in range(size)])


def shift(array, axis, step):
    size = lax.axis_size(axis)
    return lax.ppermute(array, axis, [(place, (place + step) % size) for place in range(size)])


def gather_quarters(own, axis):
    size = lax.axis_size(axis)
    pieces = {0: own}
    bit = size // 2
    while bit:
        for held in list(pieces):
            pieces[held | bit] = swap(pieces[held], axis, bit)
        bit //= 2
    return [pieces[place] for place in range(size)]


def scatter_sum(pieces, axis):
    size = lax.axis_size(axis)
    sums = {place: piece for place, piece in enumerate(pieces)}
    bit = 1
    while bit < size:
        going = [place for place in sums if place & bit]
        arrived = [swap(sums[place].astype(BF16), axis, bit) for place in going]
        for place, piece in zip(going, arrived):
            del sums[place]
            sums[place ^ bit] = sums[place ^ bit].astype(F32) + piece.astype(F32)
        bit *= 2
    return sums[0].astype(BF16)


def routing_kernel(groups, experts, me_ref, rows_ref, gain_ref, routes_ref, *outs):
    count, width = rows_ref.shape
    slots = 2 * TOPK * count // experts
    per_group = experts * slots // groups
    rotate = me_ref[0] if groups > 1 else 0
    wide = rows_ref[...].astype(F32)
    square = jnp.mean(wide * wide, axis=-1, keepdims=True)
    normed = (wide * lax.rsqrt(square + EPS) * gain_ref[...]).astype(BF16)
    row = lax.broadcasted_iota(jnp.int32, (count, count), 0)
    col = lax.broadcasted_iota(jnp.int32, (count, count), 1)
    eye = jnp.where(row == col, 1.0, 0.0).astype(BF16)
    before = jnp.where(row < col, 1.0, 0.0).astype(BF16)
    named = dot(routes_ref[...].astype(F32).astype(BF16), eye, TN)
    expert = lax.broadcasted_iota(jnp.int32, (experts, count), 0).astype(F32)
    member = named[0:1] == expert
    for k in range(1, TOPK):
        member = jnp.logical_or(member, named[k : k + 1] == expert)
    rank = dot(jnp.where(member, 1.0, 0.0).astype(BF16), before)
    rank = jnp.where(member, rank, -1.0).astype(BF16)
    for group, out_ref in enumerate(outs):
        slot = group * per_group + lax.broadcasted_iota(jnp.int32, (per_group, experts), 0)
        which = lax.broadcasted_iota(jnp.int32, (per_group, experts), 1)
        owner = lax.rem(slot // slots + rotate, experts)
        ranks = dot(jnp.where(owner == which, 1.0, 0.0).astype(BF16), rank)
        place = lax.broadcasted_iota(jnp.int32, (per_group, count), 0) % slots
        pick = jnp.where(ranks == place.astype(F32), 1.0, 0.0).astype(BF16)
        out_ref[...] = dot(pick, normed).astype(BF16)


def hidden_kernel(groups, parts, *refs):
    xs = refs[:groups]
    gates = refs[groups : groups + parts]
    ups = refs[groups + parts : groups + 2 * parts]
    out_ref = refs[groups + 2 * parts]
    x_buf, g_buf, u_buf, x_sem, g_sem, u_sem = refs[groups + 2 * parts + 1 :]
    rows = xs[0].shape[0]
    width = gates[0].shape[1]

    def x_copy(i):
        return pltpu.make_async_copy(xs[i], x_buf.at[pl.ds(i * rows, rows)], x_sem.at[i])

    def w_copy(i):
        return (
            pltpu.make_async_copy(gates[i], g_buf.at[i], g_sem.at[i]),
            pltpu.make_async_copy(ups[i], u_buf.at[i], u_sem.at[i]),
        )

    for i in range(groups):
        x_copy(i).start()
    for i in range(parts):
        for one in w_copy(i):
            one.start()
    for i in range(groups):
        x_copy(i).wait()
    for i in range(parts):
        for one in w_copy(i):
            one.wait()
        gated = dot(x_buf[...], g_buf[i])
        lifted = dot(x_buf[...], u_buf[i])
        opened = gated / (1.0 + jnp.exp(-gated))
        out_ref[:, i * width : (i + 1) * width] = (opened * lifted).astype(BF16)


def down_kernel(groups, parts, hidden_ref, *refs):
    downs = refs[:parts]
    outs = refs[parts:]
    rows = outs[0].shape[0]
    depth = downs[0].shape[0]
    total = dot(hidden_ref[:, :depth], downs[0][...])
    for i in range(1, parts):
        total += dot(hidden_ref[:, i * depth : (i + 1) * depth], downs[i][...])
    for group, out_ref in enumerate(outs):
        out_ref[...] = total[group * rows : (group + 1) * rows].astype(BF16)


def blend_kernel(groups, chunks, experts, me_ref, routes_ref, factor_ref, *refs):
    arrived = refs[: groups * chunks]
    out_ref = refs[groups * chunks]
    count = routes_ref.shape[0]
    slots = 2 * TOPK * count // experts
    per_group = experts * slots // groups
    width = arrived[0].shape[1]
    rotate = me_ref[0] if groups > 1 else 0
    row = lax.broadcasted_iota(jnp.int32, (count, count), 0)
    col = lax.broadcasted_iota(jnp.int32, (count, count), 1)
    before = jnp.where(row > col, 1.0, 0.0).astype(BF16)
    expert = lax.broadcasted_iota(jnp.int32, (count, experts), 1)
    hits = [routes_ref[:, k : k + 1] == expert for k in range(TOPK)]
    member = hits[0]
    for k in range(1, TOPK):
        member = jnp.logical_or(member, hits[k])
    rank = dot(before, jnp.where(member, 1.0, 0.0).astype(BF16))
    picks = []
    slot = lax.broadcasted_iota(jnp.int32, (count, experts * slots), 1)
    for k in range(TOPK):
        place = jnp.sum(jnp.where(hits[k], rank, 0.0), axis=1, keepdims=True).astype(jnp.int32)
        owner = lax.rem(routes_ref[:, k : k + 1] - rotate + experts, experts)
        picks.append(jnp.where(slot == owner * slots + place, 1.0, 0.0).astype(BF16))
    pick = jnp.concatenate(picks, axis=0)
    for chunk in range(chunks):
        total = None
        results = jnp.concatenate(
            [arrived[chunk * groups + group][...] for group in range(groups)], axis=0
        )
        chosen = dot(pick, results)
        for k in range(TOPK):
            term = chosen[k * count : (k + 1) * count] * factor_ref[:, k : k + 1]
            total = term if total is None else total + term
        out_ref[:, chunk * width : (chunk + 1) * width] = total.astype(BF16)


def shards(
    queries,
    forget_forward_logits,
    forget_backward_logits,
    values,
    output_gate_logits,
    lower_bound_forward,
    lower_bound_backward,
    extra_log_decay,
    head_norm_scale,
    output_projection,
    second_residual,
    expert_norm_scale,
    routes,
    specialist_mixing_factor,
    expert_gate_matrix,
    expert_up_matrix,
    expert_down_matrix,
):
    ep, tp = lax.axis_size("ep"), lax.axis_size("tp")
    direct = ep <= DIRECT_EP
    groups = ep if direct else 1
    place = jnp.stack([lax.axis_index("ep"), lax.axis_index("tp")]).astype(jnp.int32)
    rows_all, model = second_residual.shape
    count = rows_all // tp
    capacity = 2 * TOPK * count
    per_group = capacity // groups
    depth = expert_gate_matrix.shape[2]

    gates = gather_quarters(expert_gate_matrix[0], "tp")
    ups = gather_quarters(expert_up_matrix[0], "tp")
    part = model // DOWN_PARTS
    downs = [
        gather_quarters(expert_down_matrix[0, :, i * part : (i + 1) * part], "tp")
        for i in range(DOWN_PARTS)
    ]

    def own_block(grid_index, where):
        return (where[1], 0)

    def whole(grid_index, where):
        return (0, 0)

    outgoing = pl.pallas_call(
        functools.partial(routing_kernel, groups, ep),
        grid_spec=pltpu.PrefetchScalarGridSpec(
            num_scalar_prefetch=1,
            grid=(1,),
            in_specs=[
                pl.BlockSpec((count, model), own_block),
                pl.BlockSpec((1, model), whole),
                pl.BlockSpec((count, TOPK), own_block),
            ],
            out_specs=[pl.BlockSpec((per_group, model), whole)] * groups,
        ),
        out_shape=[jax.ShapeDtypeStruct((per_group, model), BF16)] * groups,
        compiler_params=params(),
        cost_estimate=cost(2 * capacity * count * model, 2 * (count + capacity) * model),
        name="routing",
    )(place, second_residual, expert_norm_scale.reshape(1, -1), routes)

    def exchange(blocks, back):
        if direct:
            return [blocks[0]] + [
                shift(blocks[step], "ep", -step if back else step) for step in range(1, ep)
            ]
        stacked = blocks[0].reshape(ep, capacity // ep, -1)
        moved = lax.all_to_all(stacked, "ep", split_axis=0, concat_axis=0, tiled=True)
        return [moved.reshape(capacity, -1)]

    arrived = exchange(outgoing, False)

    rows, key_width = queries.shape
    heads = extra_log_decay.shape[1]
    message = (key_width + 16, key_width // heads)
    shape = jax.ShapeDtypeStruct
    if direct:
        message_shapes = [shape(message, BF16)] * (ep - 1)
    else:
        message_shapes = [shape((ep,) + message, BF16)]
    local = pl.pallas_call(
        functools.partial(recurrence_kernel, ep, heads, direct),
        in_specs=[SM] + [VM] * 7,
        out_specs=[VM] * (3 + len(message_shapes)),
        out_shape=[
            shape((rows, key_width), F32),
            shape((rows, key_width), BF16),
            shape((rows, key_width), BF16),
        ]
        + message_shapes,
        scratch_shapes=[
            pltpu.VMEM((rows, rows), BF16),
            pltpu.VMEM(message, BF16),
            pltpu.VMEM(message, BF16),
        ],
        compiler_params=params(),
        cost_estimate=cost(12e9, 8 * rows * key_width, 20 * rows * key_width),
        name="recurrence",
    )(
        place,
        queries,
        forget_forward_logits,
        forget_backward_logits,
        values,
        lower_bound_forward.reshape(1, -1),
        lower_bound_backward.reshape(1, -1),
        extra_log_decay,
    )
    inner, reach_f, reach_b = local[:3]
    if direct:
        states = [shift(local[2 + step], "ep", step) for step in range(1, ep)]
    else:
        states = [lax.all_to_all(local[3], "ep", split_axis=0, concat_axis=0, tiled=True)]
    mixed = pl.pallas_call(
        functools.partial(finish_kernel, ep, tp, heads, direct),
        in_specs=[SM] + [VM] * (6 + len(states)),
        out_specs=[VM] * tp,
        out_shape=[shape((rows // tp, model), BF16)] * tp,
        scratch_shapes=[
            pltpu.VMEM((rows, key_width), BF16),
            pltpu.VMEM((key_width, key_width // heads), F32),
            pltpu.VMEM((key_width, key_width // heads), F32),
        ],
        compiler_params=params(),
        cost_estimate=cost(2 * rows * key_width * model, 6 * rows * model, rows * key_width),
        name="finish",
    )(
        place,
        inner,
        reach_f,
        reach_b,
        output_gate_logits,
        head_norm_scale.reshape(1, -1),
        output_projection,
        *states,
    )
    mixer_output = scatter_sum(mixed, "tp")

    hidden = pl.pallas_call(
        functools.partial(hidden_kernel, groups, tp),
        in_specs=[HBM] * (groups + 2 * tp),
        out_specs=VM,
        out_shape=shape((capacity, tp * depth), BF16),
        scratch_shapes=[
            pltpu.VMEM((capacity, model), BF16),
            pltpu.VMEM((tp, model, depth), BF16),
            pltpu.VMEM((tp, model, depth), BF16),
            pltpu.SemaphoreType.DMA((groups,)),
            pltpu.SemaphoreType.DMA((tp,)),
            pltpu.SemaphoreType.DMA((tp,)),
        ],
        compiler_params=params(),
        cost_estimate=cost(4 * capacity * model * tp * depth, 4 * model * tp * depth),
        name="hidden",
    )(*arrived, *gates, *ups)
    returned = []
    for i in range(DOWN_PARTS):
        results = pl.pallas_call(
            functools.partial(down_kernel, groups, tp),
            in_specs=[VM] * (1 + tp),
            out_specs=[VM] * groups,
            out_shape=[shape((per_group, part), BF16)] * groups,
            compiler_params=params(),
            cost_estimate=cost(2 * capacity * tp * depth * part, 2 * tp * depth * part),
            name=f"down_{i}",
        )(hidden, *downs[i])
        returned += exchange(results, True)
    routed_output = pl.pallas_call(
        functools.partial(blend_kernel, groups, DOWN_PARTS, ep),
        grid_spec=pltpu.PrefetchScalarGridSpec(
            num_scalar_prefetch=1,
            grid=(1,),
            in_specs=[
                pl.BlockSpec((count, TOPK), own_block),
                pl.BlockSpec((count, TOPK), whole),
            ]
            + [pl.BlockSpec((per_group, part), whole)] * (groups * DOWN_PARTS),
            out_specs=pl.BlockSpec((count, model), whole),
        ),
        out_shape=shape((count, model), BF16),
        compiler_params=params(),
        cost_estimate=cost(2 * TOPK * count * capacity * model, 2 * capacity * model),
        name="blend",
    )(place, routes, specialist_mixing_factor, *returned)
    return (mixer_output, routed_output)


def solution(mesh):
    in_specs = (
        P("ep", "tp"),
        P("ep", "tp"),
        P("ep", "tp"),
        P("ep", "tp"),
        P("ep", "tp"),
        P("tp"),
        P("tp"),
        P("ep", "tp"),
        P("tp"),
        P("tp", None),
        P("ep", None),
        P(),
        P("ep", None),
        P(("ep", "tp"), None),
        P("ep", None, "tp"),
        P("ep", None, "tp"),
        P("ep", "tp", None),
    )
    out_specs = (P(("ep", "tp"), None), P(("ep", "tp"), None))
    return jax.shard_map(shards, mesh=mesh, in_specs=in_specs, out_specs=out_specs, check_vma=False)
```

```python
import functools
import jax
import jax.numpy as jnp
from jax import lax
from jax.experimental import pallas as pl
from jax.experimental.pallas import tpu as pltpu
from jax.sharding import PartitionSpec as P

TOPK = 2
EPS = 1e-06
CHUNK = 128
FINE = 16
DIRECT_EP = 8
DOWN_PARTS = 2
F32 = jnp.float32
BF16 = jnp.bfloat16

NT = (((1,), (1,)), ((), ()))
TN = (((0,), (0,)), ((), ()))
VM = pl.BlockSpec(memory_space=pltpu.VMEM)
SM = pl.BlockSpec(memory_space=pltpu.SMEM)
HBM = pl.BlockSpec(memory_space=pl.ANY)


def cost(flops, moved, exps=0):
    return pl.CostEstimate(flops=int(flops), bytes_accessed=int(moved), transcendentals=int(exps))


def params():
    return pltpu.CompilerParams(vmem_limit_bytes=56 * 1024 * 1024)


def dot(a, b, dims=(((1,), (0,)), ((), ()))):
    return lax.dot_general(a, b, dims, preferred_element_type=F32)


def gate_terms(logits, bound, extra):
    wide = logits.astype(F32)
    grown = jnp.exp(-wide)
    opened = 1.0 / (1.0 + grown)
    floor = jax.nn.sigmoid(bound)
    rest = jax.nn.sigmoid(-bound)
    return rest * (grown * opened), jnp.log(floor + rest * opened) + extra


def running_sum(decay, lower):
    rows, width = decay.shape
    high = decay.astype(BF16)
    low = (decay - high.astype(F32)).astype(BF16)
    carry = jnp.zeros((1, width), F32)
    pieces = []
    for start in range(0, rows, CHUNK):
        both = dot(
            lower,
            jnp.concatenate([high[start : start + CHUNK], low[start : start + CHUNK]], axis=1),
        )
        piece = both[:, :width] + both[:, width:] + carry
        carry = piece[CHUNK - 1 : CHUNK]
        pieces.append(piece)
    return jnp.concatenate(pieces, axis=0)


def recurrence_kernel(
    ep, heads, direct, me_ref, q_ref, ff_ref, fb_ref, v_ref, lf_ref, lb_ref, extra_ref, *refs
):
    out_ref, reach_f_ref, reach_b_ref = refs[:3]
    message_refs = refs[3:-3]
    mix_ref, msg_f, msg_b = refs[-3:]
    rows = q_ref.shape[0]
    width = q_ref.shape[1] // heads
    tail = 16
    row = lax.broadcasted_iota(jnp.int32, (CHUNK, CHUNK), 0)
    col = lax.broadcasted_iota(jnp.int32, (CHUNK, CHUNK), 1)
    lower = jnp.where(row >= col, 1.0, 0.0).astype(BF16)
    tail_row = lax.broadcasted_iota(jnp.int32, (tail, width), 0)
    decays = [jnp.zeros((tail, width), F32), jnp.zeros((tail, width), F32)]
    for head in range(heads):
        lanes = slice(head * width, (head + 1) * width)
        q = q_ref[:, lanes].astype(F32)
        q = q / (1.0 + jnp.exp(-q))
        v = v_ref[:, lanes]
        extra = jnp.transpose(jnp.broadcast_to(extra_ref[head : head + 1, :], (width, rows)))
        kf, gf = gate_terms(ff_ref[:, lanes], lf_ref[:, lanes], extra)
        kb, gb = gate_terms(fb_ref[:, lanes], lb_ref[:, lanes], extra)
        b = running_sum(gf, lower)
        total_f = b[rows - 1 : rows]
        ahead = running_sum(gb, lower)
        total_b = ahead[rows - 1 : rows]
        c = total_b - ahead + gb

        half = rows // 2
        while half >= CHUNK:
            for first in range(0, rows, 2 * half):
                mid, last = first + half, first + 2 * half
                one, two = slice(first, mid), slice(mid, last)
                ref_f, ref_b = b[mid - 1 : mid], c[mid : mid + 1]
                mix_ref[two, one] = dot(
                    (q[two] * jnp.exp(b[two] - ref_f)).astype(BF16),
                    (kf[one] * jnp.exp(ref_f - b[one])).astype(BF16),
                    NT,
                ).astype(BF16)
                mix_ref[one, two] = dot(
                    (q[one] * jnp.exp(c[one] - ref_b)).astype(BF16),
                    (kb[two] * jnp.exp(ref_b - c[two])).astype(BF16),
                    NT,
                ).astype(BF16)
            half //= 2
        for start in range(0, rows, CHUNK):
            here = slice(start, start + CHUNK)
            qc, kfc, kbc, bc, cc = q[here], kf[here], kb[here], b[here], c[here]
            mid_f, mid_b = [], []
            for first in range(0, CHUNK, FINE):
                at = first + FINE // 2
                mid_f.append(jnp.broadcast_to(bc[at - 1 : at], (FINE, width)))
                mid_b.append(jnp.broadcast_to(cc[at : at + 1], (FINE, width)))
            df = bc - jnp.concatenate(mid_f, axis=0)
            db = cc - jnp.concatenate(mid_b, axis=0)
            near_f = dot((qc * jnp.exp(df)).astype(BF16), (kfc * jnp.exp(-df)).astype(BF16), NT)
            near_b = dot((qc * jnp.exp(db)).astype(BF16), (kbc * jnp.exp(-db)).astype(BF16), NT)
            scores = jnp.where(row >= col, near_f, 0.0) + jnp.where(row <= col, near_b, 0.0)
            half = FINE
            while half < CHUNK:
                q_side, k_side = [], []
                for first in range(0, CHUNK, 2 * half):
                    mid, last = first + half, first + 2 * half
                    one, two = slice(first, mid), slice(mid, last)
                    ref_f, ref_b = bc[mid - 1 : mid], cc[mid : mid + 1]
                    q_side.append(qc[one] * jnp.exp(cc[one] - ref_b))
                    q_side.append(qc[two] * jnp.exp(bc[two] - ref_f))
                    k_side.append(kfc[one] * jnp.exp(ref_f - bc[one]))
                    k_side.append(kbc[two] * jnp.exp(ref_b - cc[two]))
                far = dot(
                    jnp.concatenate(q_side, axis=0).astype(BF16),
                    jnp.concatenate(k_side, axis=0).astype(BF16),
                    NT,
                )
                scores = jnp.where(row // half == col // half, scores, far)
                half *= 2
            mix_ref[here, here] = scores.astype(BF16)
        out_ref[:, lanes] = dot(mix_ref[...], v)
        reach_f_ref[:, lanes] = (q * jnp.exp(b)).astype(BF16)
        reach_b_ref[:, lanes] = (q * jnp.exp(c)).astype(BF16)
        for which, message, key, run, total in (
            (0, msg_f, kf, b, total_f),
            (1, msg_b, kb, c, total_b),
        ):
            state = dot(v, (key * jnp.exp(total - run)).astype(BF16), TN)
            message[lanes, :] = state.astype(BF16)
            high = total.astype(BF16).astype(F32)
            decays[which] = jnp.where(tail_row == head, high, decays[which])
            decays[which] = jnp.where(tail_row == heads + head, total - high, decays[which])
    edge = heads * width
    msg_f[edge : edge + tail, :] = decays[0].astype(BF16)
    msg_b[edge : edge + tail, :] = decays[1].astype(BF16)
    me = me_ref[0]
    for step in range(1, ep):
        if direct:
            later = (me ^ step) > me
            target = message_refs[step - 1]

            @pl.when(later)
            def _(target=target):
                target[...] = msg_f[...]

            @pl.when(jnp.logical_not(later))
            def _(target=target):
                target[...] = msg_b[...]
    if not direct:

        def fill(place, carry):
            message_refs[0][place] = jnp.where(place > me, msg_f[...], msg_b[...])
            return carry

        lax.fori_loop(0, ep, fill, 0)


def finish_kernel(
    ep, tp, heads, direct, me_ref, quarter_ref, out_ref, reach_f_ref, reach_b_ref, gate_ref, gain_ref, w_ref, *refs
):
    count = ep - 1 if direct else 1
    arrived = refs[:count]
    pieces = refs[count : count + tp]
    hidden_ref, in_f, in_b = refs[count + tp : count + tp + 3]
    rows = out_ref.shape[0]
    width = out_ref.shape[1] // heads
    edge = heads * width
    me, quarter = me_ref[0], quarter_ref[0]
    in_f[...] = jnp.zeros_like(in_f)
    in_b[...] = jnp.zeros_like(in_b)

    def join(state_ref, read):
        decay = read(slice(edge, edge + 16)).astype(F32)
        for head in range(heads):
            lanes = slice(head * width, (head + 1) * width)
            total = decay[head : head + 1] + decay[heads + head : heads + head + 1]
            state_ref[lanes, :] = state_ref[lanes, :] * jnp.exp(total) + read(lanes).astype(F32)

    if direct:
        held_ref = refs[-1]
        for step in range(1, ep):
            held_ref[me ^ step] = arrived[step - 1][...]
    else:
        held_ref = arrived[0]

    def forward(place, carry):
        join(in_f, lambda part: held_ref[place, part, :])
        return carry

    def backward(place, carry):
        join(in_b, lambda part: held_ref[ep - 1 - place, part, :])
        return carry

    lax.fori_loop(0, me, forward, 0)
    lax.fori_loop(0, ep - 1 - me, backward, 0)
    for head in range(heads):
        lanes = slice(head * width, (head + 1) * width)
        combined = (
            out_ref[:, lanes]
            + dot(reach_f_ref[:, lanes], in_f[lanes, :].astype(BF16), NT)
            + dot(reach_b_ref[:, lanes], in_b[lanes, :].astype(BF16), NT)
        )
        square = jnp.mean(combined * combined, axis=-1, keepdims=True)
        gate = gate_ref[:, lanes].astype(F32)
        gate = gate / (1.0 + jnp.exp(-gate))
        scaled = combined * lax.rsqrt(square + EPS) * gain_ref[:, lanes]
        hidden_ref[:, lanes] = (scaled * gate).astype(BF16)
    block = rows // tp
    for piece in range(tp):
        start = pl.multiple_of((quarter ^ piece) * block, block)
        part = hidden_ref[pl.ds(start, block), :]
        pieces[piece][...] = dot(part, w_ref[...]).astype(BF16)


def swap(array, axis, bit):
    size = lax.axis_size(axis)
    return lax.ppermute(array, axis, [(place, place ^ bit) for place in range(size)])


def gather_quarters(own, axis):
    size = lax.axis_size(axis)
    pieces = {0: own}
    bit = size // 2
    while bit:
        for held in list(pieces):
            pieces[held | bit] = swap(pieces[held], axis, bit)
        bit //= 2
    return [pieces[place] for place in range(size)]


def scatter_sum(pieces, axis):
    size = lax.axis_size(axis)
    sums = {place: piece for place, piece in enumerate(pieces)}
    bit = 1
    while bit < size:
        going = [place for place in sums if place & bit]
        arrived = [swap(sums[place].astype(BF16), axis, bit) for place in going]
        for place, piece in zip(going, arrived):
            del sums[place]
            sums[place ^ bit] = sums[place ^ bit].astype(F32) + piece.astype(F32)
        bit *= 2
    return sums[0].astype(BF16)


def routing_kernel(groups, experts, me_ref, quarter_ref, rows_ref, gain_ref, routes_ref, *outs):
    count, _ = rows_ref.shape
    slots = 2 * TOPK * count // experts
    per_group = experts * slots // groups
    wide = rows_ref[...].astype(F32)
    square = jnp.mean(wide * wide, axis=-1, keepdims=True)
    normed = (wide * lax.rsqrt(square + EPS) * gain_ref[...]).astype(BF16)
    row = lax.broadcasted_iota(jnp.int32, (count, count), 0)
    col = lax.broadcasted_iota(jnp.int32, (count, count), 1)
    before = jnp.where(row < col, 1.0, 0.0).astype(BF16)
    expert = lax.broadcasted_iota(jnp.int32, (experts, count), 0)
    member = routes_ref[0:1, :] == expert
    for k in range(1, TOPK):
        member = jnp.logical_or(member, routes_ref[k : k + 1, :] == expert)
    rank = dot(jnp.where(member, 1.0, 0.0).astype(BF16), before)
    rank = jnp.where(member, rank, -1.0).astype(BF16)
    for group, out_ref in enumerate(outs):
        slot = group * per_group + lax.broadcasted_iota(jnp.int32, (per_group, experts), 0)
        which = lax.broadcasted_iota(jnp.int32, (per_group, experts), 1)
        owner = slot // slots
        if groups > 1:
            owner = owner ^ me_ref[0]
        ranks = dot(jnp.where(owner == which, 1.0, 0.0).astype(BF16), rank)
        place = lax.broadcasted_iota(jnp.int32, (per_group, count), 0) % slots
        pick = jnp.where(ranks == place.astype(F32), 1.0, 0.0).astype(BF16)
        out_ref[...] = dot(pick, normed).astype(BF16)


def hidden_kernel(groups, parts, *refs):
    xs = refs[:groups]
    gates = refs[groups : groups + parts]
    ups = refs[groups + parts : groups + 2 * parts]
    out_ref = refs[groups + 2 * parts]
    x_buf, g_buf, u_buf, x_sem, g_sem, u_sem = refs[groups + 2 * parts + 1 :]
    rows = xs[0].shape[0]
    width = gates[0].shape[1]

    def x_copy(i):
        return pltpu.make_async_copy(xs[i], x_buf.at[pl.ds(i * rows, rows)], x_sem.at[i])

    def w_copy(i):
        return (
            pltpu.make_async_copy(gates[i], g_buf.at[i], g_sem.at[i]),
            pltpu.make_async_copy(ups[i], u_buf.at[i], u_sem.at[i]),
        )

    for i in range(groups):
        x_copy(i).start()
    for i in range(parts):
        for one in w_copy(i):
            one.start()
    for i in range(groups):
        x_copy(i).wait()
    for i in range(parts):
        for one in w_copy(i):
            one.wait()
        gated = dot(x_buf[...], g_buf[i])
        lifted = dot(x_buf[...], u_buf[i])
        opened = gated / (1.0 + jnp.exp(-gated))
        out_ref[:, i * width : (i + 1) * width] = (opened * lifted).astype(BF16)


def down_kernel(groups, parts, hidden_ref, *refs):
    outs = refs[-groups:]
    downs = refs[:-groups]
    rows = outs[0].shape[0]
    depth, width = downs[0].shape
    for chunk in range(len(downs) // parts):
        total = None
        for i in range(parts):
            term = dot(hidden_ref[:, i * depth : (i + 1) * depth], downs[chunk * parts + i][...])
            total = term if total is None else total + term
        for group, out_ref in enumerate(outs):
            out_ref[:, chunk * width : (chunk + 1) * width] = total[
                group * rows : (group + 1) * rows
            ].astype(BF16)


def blend_kernel(groups, experts, me_ref, quarter_ref, routes_ref, factor_ref, *refs):
    arrived = refs[:groups]
    out_ref = refs[-1]
    count = routes_ref.shape[1]
    slots = 2 * TOPK * count // experts
    row = lax.broadcasted_iota(jnp.int32, (count, count), 0)
    col = lax.broadcasted_iota(jnp.int32, (count, count), 1)
    before = jnp.where(row > col, 1.0, 0.0).astype(BF16)

    def column(line):
        return jnp.transpose(jnp.broadcast_to(line, (count, count)))

    named = [column(routes_ref[k : k + 1, :]) for k in range(TOPK)]
    hits = [named[k] == col for k in range(TOPK)]
    member = hits[0]
    for k in range(1, TOPK):
        member = jnp.logical_or(member, hits[k])
    rank = dot(before, jnp.where(member, 1.0, 0.0).astype(BF16))
    picks = []
    slot = lax.broadcasted_iota(jnp.int32, (count, experts * slots), 1)
    for k in range(TOPK):
        place = jnp.sum(jnp.where(hits[k], rank, 0.0), axis=1, keepdims=True).astype(jnp.int32)
        owner = named[k][:, :1]
        if groups > 1:
            owner = owner ^ me_ref[0]
        picks.append(jnp.where(slot == owner * slots + place, 1.0, 0.0).astype(BF16))
    pick = jnp.concatenate(picks, axis=0)
    results = jnp.concatenate([one[...] for one in arrived], axis=0)
    chosen = dot(pick, results)
    total = None
    for k in range(TOPK):
        factor = column(factor_ref[k : k + 1, :])[:, :1]
        term = chosen[k * count : (k + 1) * count] * factor
        total = term if total is None else total + term
    width = total.shape[1]
    done = 0
    for earlier in refs[groups:-1]:
        out_ref[:, done : done + width] = earlier[...]
        done += width
    out_ref[:, done : done + width] = total.astype(BF16)


def call(kernel, operands, **options):
    return pl.pallas_call(kernel, compiler_params=params(), **options)(*operands)


def shards(
    queries,
    forget_forward_logits,
    forget_backward_logits,
    values,
    output_gate_logits,
    lower_bound_forward,
    lower_bound_backward,
    extra_log_decay,
    head_norm_scale,
    output_projection,
    second_residual,
    expert_norm_scale,
    routes,
    specialist_mixing_factor,
    expert_gate_matrix,
    expert_up_matrix,
    expert_down_matrix,
):
    ep, tp = lax.axis_size("ep"), lax.axis_size("tp")
    direct = ep <= DIRECT_EP
    groups = ep if direct else 1
    me = lax.axis_index("ep").reshape(1).astype(jnp.int32)
    quarter = lax.axis_index("tp").reshape(1).astype(jnp.int32)
    rows_all, model = second_residual.shape
    count = rows_all // tp
    capacity = 2 * TOPK * count
    per_group = capacity // groups
    depth = expert_gate_matrix.shape[2]
    shape = jax.ShapeDtypeStruct
    routes_t = routes.T
    factor_t = specialist_mixing_factor.T
    half = ep // 2
    sets = {"far": list(range(half, ep)), "near": list(range(half))} if direct else {"all": [0]}

    gates = gather_quarters(expert_gate_matrix[0], "tp")
    ups = gather_quarters(expert_up_matrix[0], "tp")
    part = model // DOWN_PARTS
    downs = [
        gather_quarters(expert_down_matrix[0, :, i * part : (i + 1) * part], "tp")
        for i in range(DOWN_PARTS)
    ]

    def whole(grid_index, a, b):
        return (0, 0)

    outgoing = call(
        functools.partial(routing_kernel, groups, ep),
        (me, quarter, second_residual, expert_norm_scale.reshape(1, -1), routes_t),
        grid_spec=pltpu.PrefetchScalarGridSpec(
            num_scalar_prefetch=2,
            grid=(1,),
            in_specs=[
                pl.BlockSpec((count, model), lambda i, a, b: (b[0], 0)),
                pl.BlockSpec((1, model), whole),
                pl.BlockSpec((TOPK, count), lambda i, a, b: (0, b[0])),
            ],
            out_specs=[pl.BlockSpec((per_group, model), whole)] * groups,
        ),
        out_shape=[shape((per_group, model), BF16)] * groups,
        cost_estimate=cost(2 * capacity * count * model, 2 * (count + capacity) * model),
    )

    def exchange(blocks):
        if direct:
            return {
                step: swap(block, "ep", step) if step else block
                for step, block in blocks.items()
            }
        stacked = blocks[0].reshape(ep, capacity // ep, -1)
        moved = lax.all_to_all(stacked, "ep", split_axis=0, concat_axis=0, tiled=True)
        return {0: moved.reshape(capacity, -1)}

    arrived = {}
    for chosen in sets.values():
        arrived.update(exchange({step: outgoing[step] for step in chosen}))

    rows, key_width = queries.shape
    heads = extra_log_decay.shape[1]
    message = (key_width + 16, key_width // heads)
    if direct:
        message_shapes = [shape(message, BF16)] * (ep - 1)
    else:
        message_shapes = [shape((ep,) + message, BF16)]
    local = call(
        functools.partial(recurrence_kernel, ep, heads, direct),
        (
            me,
            queries,
            forget_forward_logits,
            forget_backward_logits,
            values,
            lower_bound_forward.reshape(1, -1),
            lower_bound_backward.reshape(1, -1),
            extra_log_decay.T,
        ),
        in_specs=[SM] + [VM] * 7,
        out_specs=[VM] * (3 + len(message_shapes)),
        out_shape=[
            shape((rows, key_width), F32),
            shape((rows, key_width), BF16),
            shape((rows, key_width), BF16),
        ]
        + message_shapes,
        scratch_shapes=[
            pltpu.VMEM((rows, rows), BF16),
            pltpu.VMEM(message, BF16),
            pltpu.VMEM(message, BF16),
        ],
        cost_estimate=cost(12e9, 8 * rows * key_width, 20 * rows * key_width),
    )
    inner, reach_f, reach_b = local[:3]
    if direct:
        states = [swap(local[2 + step], "ep", step) for step in range(1, ep)]
    else:
        states = [lax.all_to_all(local[3], "ep", split_axis=0, concat_axis=0, tiled=True)]

    returned = [{} for _ in range(DOWN_PARTS)]
    for name, chosen in sets.items():
        size = len(chosen) * per_group
        hidden = call(
            functools.partial(hidden_kernel, len(chosen), tp),
            [arrived[step] for step in chosen] + gates + ups,
            in_specs=[HBM] * (len(chosen) + 2 * tp),
            out_specs=VM,
            out_shape=shape((size, tp * depth), BF16),
            scratch_shapes=[
                pltpu.VMEM((size, model), BF16),
                pltpu.VMEM((tp, model, depth), BF16),
                pltpu.VMEM((tp, model, depth), BF16),
                pltpu.SemaphoreType.DMA((len(chosen),)),
                pltpu.SemaphoreType.DMA((tp,)),
                pltpu.SemaphoreType.DMA((tp,)),
            ],
            cost_estimate=cost(4 * size * model * tp * depth, 4 * model * tp * depth),
        )
        batches = [list(range(DOWN_PARTS))] if name == "near" else [[i] for i in range(DOWN_PARTS)]
        for batch in batches:
            wide = part * len(batch)
            results = call(
                functools.partial(down_kernel, len(chosen), tp),
                [hidden] + [piece for i in batch for piece in downs[i]],
                in_specs=[VM] * (1 + tp * len(batch)),
                out_specs=[VM] * len(chosen),
                out_shape=[shape((per_group, wide), BF16)] * len(chosen),
                cost_estimate=cost(2 * size * tp * depth * wide, 2 * tp * depth * wide),
            )
            back = exchange(dict(zip(chosen, results)))
            for at, i in enumerate(batch):
                returned[i].update({step: (block, at) for step, block in back.items()})

    mixed = call(
        functools.partial(finish_kernel, ep, tp, heads, direct),
        (
            me,
            quarter,
            inner,
            reach_f,
            reach_b,
            output_gate_logits,
            head_norm_scale.reshape(1, -1),
            output_projection,
            *states,
        ),
        in_specs=[SM, SM] + [VM] * (6 + len(states)),
        out_specs=[VM] * tp,
        out_shape=[shape((rows // tp, model), BF16)] * tp,
        scratch_shapes=[
            pltpu.VMEM((rows, key_width), BF16),
            pltpu.VMEM((key_width, key_width // heads), F32),
            pltpu.VMEM((key_width, key_width // heads), F32),
        ]
        + ([pltpu.VMEM((ep,) + message, BF16)] if direct else []),
        cost_estimate=cost(2 * rows * key_width * model, 6 * rows * model, rows * key_width),
    )
    mixer_output = scatter_sum(mixed, "tp")

    ready = []
    for i in range(DOWN_PARTS):
        last = i == DOWN_PARTS - 1
        width = model if last else part
        blocks = [returned[i][step] for step in range(groups)]
        ready.append(
            call(
                functools.partial(blend_kernel, groups, ep),
                (
                    me,
                    quarter,
                    routes_t,
                    factor_t,
                    *[block for block, at in blocks],
                    *(ready if last else []),
                ),
                grid_spec=pltpu.PrefetchScalarGridSpec(
                    num_scalar_prefetch=2,
                    grid=(1,),
                    in_specs=[
                        pl.BlockSpec((TOPK, count), lambda i, a, b: (0, b[0])),
                        pl.BlockSpec((TOPK, count), whole),
                    ]
                    + [
                        pl.BlockSpec((per_group, part), lambda i, a, b, at=at: (0, at))
                        for block, at in blocks
                    ]
                    + [pl.BlockSpec((count, part), whole)] * (i if last else 0),
                    out_specs=pl.BlockSpec((count, width), whole),
                ),
                out_shape=shape((count, width), BF16),
                cost_estimate=cost(2 * TOPK * count * capacity * part, 2 * capacity * part),
            )
        )
    return (mixer_output, ready[-1])


def solution(mesh):
    in_specs = (
        P("ep", "tp"),
        P("ep", "tp"),
        P("ep", "tp"),
        P("ep", "tp"),
        P("ep", "tp"),
        P("tp"),
        P("tp"),
        P("ep", "tp"),
        P("tp"),
        P("tp", None),
        P("ep", None),
        P(),
        P("ep", None),
        P(("ep", "tp"), None),
        P("ep", None, "tp"),
        P("ep", None, "tp"),
        P("ep", "tp", None),
    )
    out_specs = (P(("ep", "tp"), None), P(("ep", "tp"), None))
    return jax.shard_map(shards, mesh=mesh, in_specs=in_specs, out_specs=out_specs, check_vma=False)
```

```python
import functools
import jax
import jax.numpy as jnp
from jax import lax
from jax.experimental import pallas as pl
from jax.experimental.pallas import tpu as pltpu
from jax.sharding import PartitionSpec as P

TOPK = 2
EPS = 1e-06
CHUNK = 128
FINE = 16
DIRECT_EP = 8
DOWN_EIGHTHS = (5, 3)
TILE = 256
F32 = jnp.float32
BF16 = jnp.bfloat16

NT = (((1,), (1,)), ((), ()))
TN = (((0,), (0,)), ((), ()))
VM = pl.BlockSpec(memory_space=pltpu.VMEM)
SM = pl.BlockSpec(memory_space=pltpu.SMEM)
HBM = pl.BlockSpec(memory_space=pl.ANY)


def cost(flops, moved, exps=0):
    return pl.CostEstimate(flops=int(flops), bytes_accessed=int(moved), transcendentals=int(exps))


def params(mebibytes):
    return pltpu.CompilerParams(vmem_limit_bytes=mebibytes * 1024 * 1024)


def dot(a, b, dims=(((1,), (0,)), ((), ()))):
    return lax.dot_general(a, b, dims, preferred_element_type=F32)


def gate_terms(logits, bound, extra):
    wide = logits.astype(F32)
    grown = jnp.exp(-wide)
    opened = 1.0 / (1.0 + grown)
    floor = jax.nn.sigmoid(bound)
    rest = jax.nn.sigmoid(-bound)
    return rest * (grown * opened), jnp.log(floor + rest * opened) + extra


def running_sum(decay, lower):
    rows, width = decay.shape
    high = decay.astype(BF16)
    low = (decay - high.astype(F32)).astype(BF16)
    carry = jnp.zeros((1, width), F32)
    pieces = []
    for start in range(0, rows, CHUNK):
        both = dot(
            lower,
            jnp.concatenate([high[start : start + CHUNK], low[start : start + CHUNK]], axis=1),
        )
        piece = both[:, :width] + both[:, width:] + carry
        carry = piece[CHUNK - 1 : CHUNK]
        pieces.append(piece)
    return jnp.concatenate(pieces, axis=0)


TAIL = 16


def recurrence_kernel(
    heads,
    q_ref,
    ff_ref,
    fb_ref,
    v_ref,
    lf_ref,
    lb_ref,
    extra_ref,
    out_ref,
    reach_f_ref,
    reach_b_ref,
    total_ref,
    mix_ref,
):
    rows = q_ref.shape[0]
    width = q_ref.shape[1] // heads
    row = lax.broadcasted_iota(jnp.int32, (CHUNK, CHUNK), 0)
    col = lax.broadcasted_iota(jnp.int32, (CHUNK, CHUNK), 1)
    lower = jnp.where(row >= col, 1.0, 0.0).astype(BF16)
    decays = [[], []]
    for head in range(heads):
        lanes = slice(head * width, (head + 1) * width)
        q = q_ref[:, lanes].astype(F32)
        q = q / (1.0 + jnp.exp(-q))
        v = v_ref[:, lanes]
        extra = jnp.transpose(jnp.broadcast_to(extra_ref[head : head + 1, :], (width, rows)))
        kf, gf = gate_terms(ff_ref[:, lanes], lf_ref[:, lanes], extra)
        kb, gb = gate_terms(fb_ref[:, lanes], lb_ref[:, lanes], extra)
        b = running_sum(gf, lower)
        total_f = b[rows - 1 : rows]
        ahead = running_sum(gb, lower)
        total_b = ahead[rows - 1 : rows]
        c = total_b - ahead + gb

        half = rows // 2
        while half >= CHUNK:
            for first in range(0, rows, 2 * half):
                mid, last = first + half, first + 2 * half
                one, two = slice(first, mid), slice(mid, last)
                ref_f, ref_b = b[mid - 1 : mid], c[mid : mid + 1]
                mix_ref[two, one] = dot(
                    (q[two] * jnp.exp(b[two] - ref_f)).astype(BF16),
                    (kf[one] * jnp.exp(ref_f - b[one])).astype(BF16),
                    NT,
                ).astype(BF16)
                mix_ref[one, two] = dot(
                    (q[one] * jnp.exp(c[one] - ref_b)).astype(BF16),
                    (kb[two] * jnp.exp(ref_b - c[two])).astype(BF16),
                    NT,
                ).astype(BF16)
            half //= 2
        for start in range(0, rows, CHUNK):
            here = slice(start, start + CHUNK)
            qc, kfc, kbc, bc, cc = q[here], kf[here], kb[here], b[here], c[here]
            mid_f, mid_b = [], []
            for first in range(0, CHUNK, FINE):
                at = first + FINE // 2
                mid_f.append(jnp.broadcast_to(bc[at - 1 : at], (FINE, width)))
                mid_b.append(jnp.broadcast_to(cc[at : at + 1], (FINE, width)))
            df = bc - jnp.concatenate(mid_f, axis=0)
            db = cc - jnp.concatenate(mid_b, axis=0)
            near_f = dot((qc * jnp.exp(df)).astype(BF16), (kfc * jnp.exp(-df)).astype(BF16), NT)
            near_b = dot((qc * jnp.exp(db)).astype(BF16), (kbc * jnp.exp(-db)).astype(BF16), NT)
            scores = jnp.where(row >= col, near_f, 0.0) + jnp.where(row <= col, near_b, 0.0)
            half = FINE
            while half < CHUNK:
                q_side, k_side = [], []
                for first in range(0, CHUNK, 2 * half):
                    mid, last = first + half, first + 2 * half
                    one, two = slice(first, mid), slice(mid, last)
                    ref_f, ref_b = bc[mid - 1 : mid], cc[mid : mid + 1]
                    q_side.append(qc[one] * jnp.exp(cc[one] - ref_b))
                    q_side.append(qc[two] * jnp.exp(bc[two] - ref_f))
                    k_side.append(kfc[one] * jnp.exp(ref_f - bc[one]))
                    k_side.append(kbc[two] * jnp.exp(ref_b - cc[two]))
                far = dot(
                    jnp.concatenate(q_side, axis=0).astype(BF16),
                    jnp.concatenate(k_side, axis=0).astype(BF16),
                    NT,
                )
                scores = jnp.where(row // half == col // half, scores, far)
                half *= 2
            mix_ref[here, here] = scores.astype(BF16)
        out_ref[:, lanes] = dot(mix_ref[...], v)
        reach_f_ref[:, lanes] = (q * jnp.exp(b)).astype(BF16)
        reach_b_ref[:, lanes] = (q * jnp.exp(c)).astype(BF16)
        for which, key, run, total in ((0, kf, b, total_f), (1, kb, c, total_b)):
            state = dot(v, (key * jnp.exp(total - run)).astype(BF16), TN)
            total_ref[which, lanes, :] = state.astype(BF16)
            decays[which].append(total)
    for which in range(2):
        put_decays(total_ref.at[which], decays[which])


def put_decays(message_ref, decays):
    heads = len(decays)
    edge, width = message_ref.shape[0] - TAIL, message_ref.shape[1]
    row = lax.broadcasted_iota(jnp.int32, (TAIL, width), 0)
    block = jnp.zeros((TAIL, width), F32)
    for head, decay in enumerate(decays):
        high = decay.astype(BF16).astype(F32)
        block = jnp.where(row == head, high, block)
        block = jnp.where(row == heads + head, decay - high, block)
    message_ref[edge:, :] = block.astype(BF16)


def get_decays(message, heads):
    block = message[message.shape[0] - TAIL :, :].astype(F32)
    return [block[head : head + 1] + block[heads + head : heads + head + 1] for head in range(heads)]


def join_kernel(bit, heads, first, single, me_ref, own_ref, other_ref, *refs):
    if first:
        send_ref, before_ref = refs
    else:
        old_ref, send_ref, before_ref = refs
    width = own_ref.shape[2]
    edge = heads * width
    upper = (me_ref[0] & bit) != 0
    send_back = (me_ref[0] & (2 * bit)) != 0
    zero = jnp.zeros((1, width), F32)
    for which in range(2):
        own, other = own_ref[which], other_ref[which]
        own_decay, other_decay = get_decays(own, heads), get_decays(other, heads)
        leads = upper if which == 0 else jnp.logical_not(upper)
        out = send_ref if single else send_ref.at[which]
        write = send_back if which == 1 else jnp.logical_not(send_back)
        tail_row = lax.broadcasted_iota(jnp.int32, (TAIL, width), 0)
        tail = jnp.zeros((TAIL, width), F32)
        both = []
        for head in range(heads):
            lanes = slice(head * width, (head + 1) * width)
            mine, theirs = own[lanes].astype(F32), other[lanes].astype(F32)
            late = jnp.where(leads, own_decay[head], other_decay[head])
            early_state = jnp.where(leads, theirs, mine)
            late_state = jnp.where(leads, mine, theirs)
            both.append((jnp.exp(late) * early_state + late_state).astype(BF16))
            held_decay = zero if first else old_ref[which, edge + head : edge + head + 1, :]
            held = jnp.zeros_like(mine) if first else old_ref[which, lanes, :]
            passed = jnp.exp(held_decay) * theirs + held
            before_ref[which, lanes, :] = jnp.where(leads, passed, held)
            reach = jnp.where(leads, held_decay + other_decay[head], held_decay)
            tail = jnp.where(tail_row == head, reach, tail)
        before_ref[which, edge:, :] = tail
        sums = [mine + theirs for mine, theirs in zip(own_decay, other_decay)]

        def put(out=out, both=both, sums=sums):
            for head in range(heads):
                out[head * width : (head + 1) * width, :] = both[head]
            put_decays(out, sums)

        if single:
            pl.when(write)(put)
        else:
            put()


def finish_kernel(
    bit,
    tp,
    heads,
    me_ref,
    quarter_ref,
    out_ref,
    reach_f_ref,
    reach_b_ref,
    gate_ref,
    gain_ref,
    w_ref,
    other_ref,
    before_ref,
    *refs,
):
    pieces = refs[:tp]
    hidden_ref = refs[tp]
    rows = out_ref.shape[0]
    width = out_ref.shape[1] // heads
    edge = heads * width
    quarter = quarter_ref[0]
    upper = (me_ref[0] & bit) != 0
    for head in range(heads):
        lanes = slice(head * width, (head + 1) * width)
        other = other_ref[lanes, :].astype(F32)
        combined = out_ref[:, lanes]
        for which, reach_ref in ((0, reach_f_ref), (1, reach_b_ref)):
            leads = upper if which == 0 else jnp.logical_not(upper)
            held = before_ref[which, lanes, :]
            passed = jnp.exp(before_ref[which, edge + head : edge + head + 1, :]) * other + held
            incoming = jnp.where(leads, passed, held).astype(BF16)
            combined += dot(reach_ref[:, lanes], incoming, NT)
        square = jnp.mean(combined * combined, axis=-1, keepdims=True)
        gate = gate_ref[:, lanes].astype(F32)
        gate = gate / (1.0 + jnp.exp(-gate))
        scaled = combined * lax.rsqrt(square + EPS) * gain_ref[:, lanes]
        hidden_ref[:, lanes] = (scaled * gate).astype(BF16)
    block = rows // tp
    for piece in range(tp):
        start = pl.multiple_of((quarter ^ piece) * block, block)
        part = hidden_ref[pl.ds(start, block), :]
        pieces[piece][...] = dot(part, w_ref[...]).astype(BF16)


def swap(array, axis, bit):
    size = lax.axis_size(axis)
    return lax.ppermute(array, axis, [(place, place ^ bit) for place in range(size)])


def gather_quarters(own, axis):
    size = lax.axis_size(axis)
    pieces = {0: own}
    bit = size // 2
    while bit:
        for held in list(pieces):
            pieces[held | bit] = swap(pieces[held], axis, bit)
        bit //= 2
    return [pieces[place] for place in range(size)]


def scatter_sum(pieces, axis):
    size = lax.axis_size(axis)
    sums = {place: piece for place, piece in enumerate(pieces)}
    bit = 1
    while bit < size:
        going = [place for place in sums if place & bit]
        arrived = [swap(sums[place].astype(BF16), axis, bit) for place in going]
        for place, piece in zip(going, arrived):
            del sums[place]
            sums[place ^ bit] = sums[place ^ bit].astype(F32) + piece.astype(F32)
        bit *= 2
    return sums[0].astype(BF16)


def routing_kernel(groups, experts, me_ref, quarter_ref, rows_ref, gain_ref, routes_ref, *outs):
    count, _ = rows_ref.shape
    slots = 2 * TOPK * count // experts
    per_group = experts * slots // groups
    wide = rows_ref[...].astype(F32)
    square = jnp.mean(wide * wide, axis=-1, keepdims=True)
    normed = (wide * lax.rsqrt(square + EPS) * gain_ref[...]).astype(BF16)
    row = lax.broadcasted_iota(jnp.int32, (count, count), 0)
    col = lax.broadcasted_iota(jnp.int32, (count, count), 1)
    before = jnp.where(row < col, 1.0, 0.0).astype(BF16)
    expert = lax.broadcasted_iota(jnp.int32, (experts, count), 0)
    member = routes_ref[0:1, :] == expert
    for k in range(1, TOPK):
        member = jnp.logical_or(member, routes_ref[k : k + 1, :] == expert)
    rank = dot(jnp.where(member, 1.0, 0.0).astype(BF16), before)
    rank = jnp.where(member, rank, -1.0).astype(BF16)
    for group, out_ref in enumerate(outs):
        slot = group * per_group + lax.broadcasted_iota(jnp.int32, (per_group, experts), 0)
        which = lax.broadcasted_iota(jnp.int32, (per_group, experts), 1)
        owner = slot // slots
        if groups > 1:
            owner = owner ^ me_ref[0]
        ranks = dot(jnp.where(owner == which, 1.0, 0.0).astype(BF16), rank)
        place = lax.broadcasted_iota(jnp.int32, (per_group, count), 0) % slots
        pick = jnp.where(ranks == place.astype(F32), 1.0, 0.0).astype(BF16)
        out_ref[...] = dot(pick, normed).astype(BF16)


def picks_kernel(groups, experts, me_ref, quarter_ref, routes_ref, factor_ref, pick_ref, weight_ref):
    count = routes_ref.shape[1]
    slots = 2 * TOPK * count // experts
    row = lax.broadcasted_iota(jnp.int32, (count, count), 0)
    col = lax.broadcasted_iota(jnp.int32, (count, count), 1)
    before = jnp.where(row > col, 1.0, 0.0).astype(BF16)

    def column(line):
        return jnp.transpose(jnp.broadcast_to(line, (count, count)))

    named = [column(routes_ref[k : k + 1, :]) for k in range(TOPK)]
    hits = [named[k] == col for k in range(TOPK)]
    member = hits[0]
    for k in range(1, TOPK):
        member = jnp.logical_or(member, hits[k])
    rank = dot(before, jnp.where(member, 1.0, 0.0).astype(BF16))
    slot = lax.broadcasted_iota(jnp.int32, (count, experts * slots), 1)
    for k in range(TOPK):
        place = jnp.sum(jnp.where(hits[k], rank, 0.0), axis=1, keepdims=True).astype(jnp.int32)
        owner = named[k][:, :1]
        if groups > 1:
            owner = owner ^ me_ref[0]
        rows = slice(k * count, (k + 1) * count)
        pick_ref[rows, :] = jnp.where(slot == owner * slots + place, 1.0, 0.0).astype(BF16)
        weight_ref[rows, :] = column(factor_ref[k : k + 1, :])


def hidden_kernel(groups, parts, *refs):
    xs = refs[:groups]
    gates = refs[groups : groups + parts]
    ups = refs[groups + parts : groups + 2 * parts]
    out_ref = refs[-1]
    width = gates[0].shape[1]
    x = jnp.concatenate([one[...] for one in xs], axis=0)
    for i in range(parts):
        gated = dot(x, gates[i][...])
        lifted = dot(x, ups[i][...])
        opened = gated / (1.0 + jnp.exp(-gated))
        out_ref[:, i * width : (i + 1) * width] = (opened * lifted).astype(BF16)


def down_kernel(groups, parts, hidden_ref, *refs):
    downs, outs = refs[:parts], refs[parts:]
    depth, width = downs[0].shape
    rows = hidden_ref.shape[0] // groups
    for first in range(0, width, TILE):
        lanes = slice(first, min(first + TILE, width))
        total = None
        for i in range(parts):
            term = dot(hidden_ref[:, i * depth : (i + 1) * depth], downs[i][:, lanes])
            total = term if total is None else total + term
        result = total.astype(BF16)
        for group, out_ref in enumerate(outs):
            out_ref[:, lanes] = result[group * rows : (group + 1) * rows]


def blend_kernel(groups, pick_ref, weight_ref, *refs):
    arrived = refs[:groups]
    out_ref = refs[-1]
    count = out_ref.shape[0]
    results = jnp.concatenate([one[...] for one in arrived], axis=0)
    chosen = dot(pick_ref[...], results)
    total = None
    for k in range(TOPK):
        rows = slice(k * count, (k + 1) * count)
        term = chosen[rows] * weight_ref[rows, :1]
        total = term if total is None else total + term
    done = 0
    for earlier in refs[groups:-1]:
        out_ref[:, done : done + earlier.shape[1]] = earlier[...]
        done += earlier.shape[1]
    out_ref[:, done : done + total.shape[1]] = total.astype(BF16)


def call(kernel, operands, room=12, **options):
    return pl.pallas_call(kernel, compiler_params=params(room), **options)(*operands)


def shards(
    queries,
    forget_forward_logits,
    forget_backward_logits,
    values,
    output_gate_logits,
    lower_bound_forward,
    lower_bound_backward,
    extra_log_decay,
    head_norm_scale,
    output_projection,
    second_residual,
    expert_norm_scale,
    routes,
    specialist_mixing_factor,
    expert_gate_matrix,
    expert_up_matrix,
    expert_down_matrix,
):
    ep, tp = lax.axis_size("ep"), lax.axis_size("tp")
    direct = ep <= DIRECT_EP
    groups = ep if direct else 1
    me = lax.axis_index("ep").reshape(1).astype(jnp.int32)
    quarter = lax.axis_index("tp").reshape(1).astype(jnp.int32)
    rows_all, model = second_residual.shape
    count = rows_all // tp
    capacity = 2 * TOPK * count
    per_group = capacity // groups
    depth = expert_gate_matrix.shape[2]
    shape = jax.ShapeDtypeStruct
    routes_t = routes.T
    factor_t = specialist_mixing_factor.T

    gates = gather_quarters(expert_gate_matrix[0], "tp")
    ups = gather_quarters(expert_up_matrix[0], "tp")
    edges = [0]
    for share in DOWN_EIGHTHS:
        edges.append(edges[-1] + model * share // sum(DOWN_EIGHTHS))
    parts = list(zip(edges, edges[1:]))
    downs = [gather_quarters(expert_down_matrix[0, :, start:stop], "tp") for start, stop in parts]

    def whole(grid_index, a, b):
        return (0, 0)

    outgoing = call(
        functools.partial(routing_kernel, groups, ep),
        (me, quarter, second_residual, expert_norm_scale.reshape(1, -1), routes_t),
        grid_spec=pltpu.PrefetchScalarGridSpec(
            num_scalar_prefetch=2,
            grid=(1,),
            in_specs=[
                pl.BlockSpec((count, model), lambda i, a, b: (b[0], 0)),
                pl.BlockSpec((1, model), whole),
                pl.BlockSpec((TOPK, count), lambda i, a, b: (0, b[0])),
            ],
            out_specs=[pl.BlockSpec((per_group, model), whole)] * groups,
        ),
        out_shape=[shape((per_group, model), BF16)] * groups,
        cost_estimate=cost(2 * capacity * count * model, 2 * (count + capacity) * model),
    )

    def exchange(blocks):
        if direct:
            return {
                step: swap(block, "ep", step) if step else block
                for step, block in blocks.items()
            }
        stacked = blocks[0].reshape(ep, capacity // ep, -1)
        moved = lax.all_to_all(stacked, "ep", split_axis=0, concat_axis=0, tiled=True)
        return {0: moved.reshape(capacity, -1)}

    arrived = exchange(dict(enumerate(outgoing)))

    rows, key_width = queries.shape
    heads = extra_log_decay.shape[1]
    message = (key_width + TAIL, key_width // heads)
    inner, reach_f, reach_b, total = call(
        functools.partial(recurrence_kernel, heads),
        (
            queries,
            forget_forward_logits,
            forget_backward_logits,
            values,
            lower_bound_forward.reshape(1, -1),
            lower_bound_backward.reshape(1, -1),
            extra_log_decay.T,
        ),
        in_specs=[VM] * 7,
        out_specs=[VM] * 4,
        out_shape=[
            shape((rows, key_width), F32),
            shape((rows, key_width), BF16),
            shape((rows, key_width), BF16),
            shape((2,) + message, BF16),
        ],
        scratch_shapes=[pltpu.VMEM((rows, rows), BF16)],
        cost_estimate=cost(12e9, 8 * rows * key_width, 20 * rows * key_width),
    )
    bit = 1
    before = None
    while bit < ep:
        other = swap(total, "ep", bit)
        if 2 * bit < ep:
            single = 4 * bit >= ep
            total, before = call(
                functools.partial(join_kernel, bit, heads, before is None, single),
                (me, total, other) + (() if before is None else (before,)),
                in_specs=[SM] + [VM] * (2 if before is None else 3),
                out_specs=[VM] * 2,
                out_shape=[
                    shape(message if single else (2,) + message, BF16),
                    shape((2,) + message, F32),
                ],
                cost_estimate=cost(4 * key_width * key_width, 8 * key_width * key_width),
            )
        bit *= 2

    hidden = call(
        functools.partial(hidden_kernel, groups, tp),
        [arrived[step] for step in range(groups)] + gates + ups,
        room=24,
        in_specs=[VM] * (groups + 2 * tp),
        out_specs=VM,
        out_shape=shape((capacity, tp * depth), BF16),
        cost_estimate=cost(4 * capacity * model * tp * depth, 4 * model * tp * depth),
    )
    returned = []
    for i, (start, stop) in enumerate(parts):
        wide = stop - start
        results = call(
            functools.partial(down_kernel, groups, tp),
            [hidden] + downs[i],
            in_specs=[VM] * (1 + tp),
            out_specs=[VM] * groups,
            out_shape=[shape((per_group, wide), BF16)] * groups,
            cost_estimate=cost(2 * capacity * tp * depth * wide, 2 * tp * depth * wide),
        )
        returned.append(exchange(dict(enumerate(results))))

    mixed = call(
        functools.partial(finish_kernel, ep // 2, tp, heads),
        (
            me,
            quarter,
            inner,
            reach_f,
            reach_b,
            output_gate_logits,
            head_norm_scale.reshape(1, -1),
            output_projection,
            other,
            before,
        ),
        in_specs=[SM, SM] + [VM] * 8,
        out_specs=[VM] * tp,
        out_shape=[shape((rows // tp, model), BF16)] * tp,
        scratch_shapes=[pltpu.VMEM((rows, key_width), BF16)],
        cost_estimate=cost(2 * rows * key_width * model, 6 * rows * model, rows * key_width),
    )
    mixer_output = scatter_sum(mixed, "tp")

    pick, weight = call(
        functools.partial(picks_kernel, groups, ep),
        (me, quarter, routes_t, factor_t),
        grid_spec=pltpu.PrefetchScalarGridSpec(
            num_scalar_prefetch=2,
            grid=(1,),
            in_specs=[
                pl.BlockSpec((TOPK, count), lambda i, a, b: (0, b[0])),
                pl.BlockSpec((TOPK, count), whole),
            ],
            out_specs=[
                pl.BlockSpec((TOPK * count, capacity), whole),
                pl.BlockSpec((TOPK * count, count), whole),
            ],
        ),
        out_shape=[shape((TOPK * count, capacity), BF16), shape((TOPK * count, count), F32)],
        cost_estimate=cost(4 * count * count * count, 2 * TOPK * count * capacity),
    )
    ready = []
    for i, (start, stop) in enumerate(parts):
        last = i == len(parts) - 1
        if last:
            pick, mixer_output = lax.optimization_barrier((pick, mixer_output))
        blocks = [returned[i][step] for step in range(groups)]
        ready.append(
            call(
                functools.partial(blend_kernel, groups),
                (pick, weight, *blocks, *(ready if last else [])),
                in_specs=[VM] * (2 + groups + (i if last else 0)),
                out_specs=VM,
                out_shape=shape((count, model if last else stop - start), BF16),
                cost_estimate=cost(
                    2 * TOPK * count * capacity * (stop - start), 2 * capacity * (stop - start)
                ),
            )
        )
    return (mixer_output, ready[-1])


def solution(mesh):
    in_specs = (
        P("ep", "tp"),
        P("ep", "tp"),
        P("ep", "tp"),
        P("ep", "tp"),
        P("ep", "tp"),
        P("tp"),
        P("tp"),
        P("ep", "tp"),
        P("tp"),
        P("tp", None),
        P("ep", None),
        P(),
        P("ep", None),
        P(("ep", "tp"), None),
        P("ep", None, "tp"),
        P("ep", None, "tp"),
        P("ep", "tp", None),
    )
    out_specs = (P(("ep", "tp"), None), P(("ep", "tp"), None))
    return jax.shard_map(shards, mesh=mesh, in_specs=in_specs, out_specs=out_specs, check_vma=False)
```

```python
import functools
import jax
import jax.numpy as jnp
from jax import lax
from jax.experimental import pallas as pl
from jax.experimental.pallas import tpu as pltpu
from jax.sharding import PartitionSpec as P

TOPK = 2
EPS = 1e-06
CHUNK = 128
FINE = 16
DIRECT_EP = 8
DOWN_EIGHTHS = (3, 3, 2)
TILE = 256
F32 = jnp.float32
BF16 = jnp.bfloat16

NT = (((1,), (1,)), ((), ()))
TN = (((0,), (0,)), ((), ()))
VM = pl.BlockSpec(memory_space=pltpu.VMEM)
SM = pl.BlockSpec(memory_space=pltpu.SMEM)
HBM = pl.BlockSpec(memory_space=pl.ANY)


def cost(flops, moved, exps=0):
    return pl.CostEstimate(flops=int(flops), bytes_accessed=int(moved), transcendentals=int(exps))


def params(mebibytes):
    return pltpu.CompilerParams(vmem_limit_bytes=mebibytes * 1024 * 1024)


def dot(a, b, dims=(((1,), (0,)), ((), ()))):
    return lax.dot_general(a, b, dims, preferred_element_type=F32)


def gate_terms(logits, bound, extra):
    wide = logits.astype(F32)
    grown = jnp.exp(-wide)
    opened = 1.0 / (1.0 + grown)
    floor = jax.nn.sigmoid(bound)
    rest = jax.nn.sigmoid(-bound)
    return rest * (grown * opened), jnp.log(floor + rest * opened) + extra


def running_sum(decay, lower):
    rows, width = decay.shape
    high = decay.astype(BF16)
    low = (decay - high.astype(F32)).astype(BF16)
    carry = jnp.zeros((1, width), F32)
    pieces = []
    for start in range(0, rows, CHUNK):
        both = dot(
            lower,
            jnp.concatenate([high[start : start + CHUNK], low[start : start + CHUNK]], axis=1),
        )
        piece = both[:, :width] + both[:, width:] + carry
        carry = piece[CHUNK - 1 : CHUNK]
        pieces.append(piece)
    return jnp.concatenate(pieces, axis=0)


TAIL = 16


def recurrence_kernel(
    heads,
    q_ref,
    ff_ref,
    fb_ref,
    v_ref,
    lf_ref,
    lb_ref,
    extra_ref,
    out_ref,
    reach_f_ref,
    reach_b_ref,
    total_ref,
    mix_ref,
):
    rows = q_ref.shape[0]
    width = q_ref.shape[1] // heads
    row = lax.broadcasted_iota(jnp.int32, (CHUNK, CHUNK), 0)
    col = lax.broadcasted_iota(jnp.int32, (CHUNK, CHUNK), 1)
    lower = jnp.where(row >= col, 1.0, 0.0).astype(BF16)
    decays = [[], []]
    for head in range(heads):
        lanes = slice(head * width, (head + 1) * width)
        q = q_ref[:, lanes].astype(F32)
        q = q / (1.0 + jnp.exp(-q))
        v = v_ref[:, lanes]
        extra = jnp.transpose(jnp.broadcast_to(extra_ref[head : head + 1, :], (width, rows)))
        kf, gf = gate_terms(ff_ref[:, lanes], lf_ref[:, lanes], extra)
        kb, gb = gate_terms(fb_ref[:, lanes], lb_ref[:, lanes], extra)
        b = running_sum(gf, lower)
        total_f = b[rows - 1 : rows]
        ahead = running_sum(gb, lower)
        total_b = ahead[rows - 1 : rows]
        c = total_b - ahead + gb

        half = rows // 2
        while half >= CHUNK:
            for first in range(0, rows, 2 * half):
                mid, last = first + half, first + 2 * half
                one, two = slice(first, mid), slice(mid, last)
                ref_f, ref_b = b[mid - 1 : mid], c[mid : mid + 1]
                mix_ref[two, one] = dot(
                    (q[two] * jnp.exp(b[two] - ref_f)).astype(BF16),
                    (kf[one] * jnp.exp(ref_f - b[one])).astype(BF16),
                    NT,
                ).astype(BF16)
                mix_ref[one, two] = dot(
                    (q[one] * jnp.exp(c[one] - ref_b)).astype(BF16),
                    (kb[two] * jnp.exp(ref_b - c[two])).astype(BF16),
                    NT,
                ).astype(BF16)
            half //= 2
        for start in range(0, rows, CHUNK):
            here = slice(start, start + CHUNK)
            qc, kfc, kbc, bc, cc = q[here], kf[here], kb[here], b[here], c[here]
            mid_f, mid_b = [], []
            for first in range(0, CHUNK, FINE):
                at = first + FINE // 2
                mid_f.append(jnp.broadcast_to(bc[at - 1 : at], (FINE, width)))
                mid_b.append(jnp.broadcast_to(cc[at : at + 1], (FINE, width)))
            df = bc - jnp.concatenate(mid_f, axis=0)
            db = cc - jnp.concatenate(mid_b, axis=0)
            near_f = dot((qc * jnp.exp(df)).astype(BF16), (kfc * jnp.exp(-df)).astype(BF16), NT)
            near_b = dot((qc * jnp.exp(db)).astype(BF16), (kbc * jnp.exp(-db)).astype(BF16), NT)
            scores = jnp.where(row >= col, near_f, 0.0) + jnp.where(row <= col, near_b, 0.0)
            half = FINE
            while half < CHUNK:
                q_side, k_side = [], []
                for first in range(0, CHUNK, 2 * half):
                    mid, last = first + half, first + 2 * half
                    one, two = slice(first, mid), slice(mid, last)
                    ref_f, ref_b = bc[mid - 1 : mid], cc[mid : mid + 1]
                    q_side.append(qc[one] * jnp.exp(cc[one] - ref_b))
                    q_side.append(qc[two] * jnp.exp(bc[two] - ref_f))
                    k_side.append(kfc[one] * jnp.exp(ref_f - bc[one]))
                    k_side.append(kbc[two] * jnp.exp(ref_b - cc[two]))
                far = dot(
                    jnp.concatenate(q_side, axis=0).astype(BF16),
                    jnp.concatenate(k_side, axis=0).astype(BF16),
                    NT,
                )
                scores = jnp.where(row // half == col // half, scores, far)
                half *= 2
            mix_ref[here, here] = scores.astype(BF16)
        out_ref[:, lanes] = dot(mix_ref[...], v)
        reach_f_ref[:, lanes] = (q * jnp.exp(b)).astype(BF16)
        reach_b_ref[:, lanes] = (q * jnp.exp(c)).astype(BF16)
        for which, key, run, total in ((0, kf, b, total_f), (1, kb, c, total_b)):
            state = dot(v, (key * jnp.exp(total - run)).astype(BF16), TN)
            total_ref[which, lanes, :] = state.astype(BF16)
            decays[which].append(total)
    for which in range(2):
        put_decays(total_ref.at[which], decays[which])


def put_decays(message_ref, decays):
    heads = len(decays)
    edge, width = message_ref.shape[0] - TAIL, message_ref.shape[1]
    row = lax.broadcasted_iota(jnp.int32, (TAIL, width), 0)
    block = jnp.zeros((TAIL, width), F32)
    for head, decay in enumerate(decays):
        high = decay.astype(BF16).astype(F32)
        block = jnp.where(row == head, high, block)
        block = jnp.where(row == heads + head, decay - high, block)
    message_ref[edge:, :] = block.astype(BF16)


def get_decays(message, heads):
    block = message[message.shape[0] - TAIL :, :].astype(F32)
    return [block[head : head + 1] + block[heads + head : heads + head + 1] for head in range(heads)]


def join_kernel(bit, heads, first, single, me_ref, own_ref, other_ref, *refs):
    if first:
        send_ref, before_ref = refs
    else:
        old_ref, send_ref, before_ref = refs
    width = own_ref.shape[2]
    edge = heads * width
    upper = (me_ref[0] & bit) != 0
    send_back = (me_ref[0] & (2 * bit)) != 0
    zero = jnp.zeros((1, width), F32)
    for which in range(2):
        own, other = own_ref[which], other_ref[which]
        own_decay, other_decay = get_decays(own, heads), get_decays(other, heads)
        leads = upper if which == 0 else jnp.logical_not(upper)
        out = send_ref if single else send_ref.at[which]
        write = send_back if which == 1 else jnp.logical_not(send_back)
        tail_row = lax.broadcasted_iota(jnp.int32, (TAIL, width), 0)
        tail = jnp.zeros((TAIL, width), F32)
        both = []
        for head in range(heads):
            lanes = slice(head * width, (head + 1) * width)
            mine, theirs = own[lanes].astype(F32), other[lanes].astype(F32)
            late = jnp.where(leads, own_decay[head], other_decay[head])
            early_state = jnp.where(leads, theirs, mine)
            late_state = jnp.where(leads, mine, theirs)
            both.append((jnp.exp(late) * early_state + late_state).astype(BF16))
            held_decay = zero if first else old_ref[which, edge + head : edge + head + 1, :]
            held = jnp.zeros_like(mine) if first else old_ref[which, lanes, :]
            passed = jnp.exp(held_decay) * theirs + held
            before_ref[which, lanes, :] = jnp.where(leads, passed, held)
            reach = jnp.where(leads, held_decay + other_decay[head], held_decay)
            tail = jnp.where(tail_row == head, reach, tail)
        before_ref[which, edge:, :] = tail
        sums = [mine + theirs for mine, theirs in zip(own_decay, other_decay)]

        def put(out=out, both=both, sums=sums):
            for head in range(heads):
                out[head * width : (head + 1) * width, :] = both[head]
            put_decays(out, sums)

        if single:
            pl.when(write)(put)
        else:
            put()


def finish_kernel(
    bit,
    tp,
    heads,
    me_ref,
    quarter_ref,
    out_ref,
    reach_f_ref,
    reach_b_ref,
    gate_ref,
    gain_ref,
    w_ref,
    other_ref,
    before_ref,
    *refs,
):
    pieces = refs[:tp]
    hidden_ref = refs[tp]
    rows = out_ref.shape[0]
    width = out_ref.shape[1] // heads
    edge = heads * width
    quarter = quarter_ref[0]
    upper = (me_ref[0] & bit) != 0
    for head in range(heads):
        lanes = slice(head * width, (head + 1) * width)
        other = other_ref[lanes, :].astype(F32)
        combined = out_ref[:, lanes]
        for which, reach_ref in ((0, reach_f_ref), (1, reach_b_ref)):
            leads = upper if which == 0 else jnp.logical_not(upper)
            held = before_ref[which, lanes, :]
            passed = jnp.exp(before_ref[which, edge + head : edge + head + 1, :]) * other + held
            incoming = jnp.where(leads, passed, held).astype(BF16)
            combined += dot(reach_ref[:, lanes], incoming, NT)
        square = jnp.mean(combined * combined, axis=-1, keepdims=True)
        gate = gate_ref[:, lanes].astype(F32)
        gate = gate / (1.0 + jnp.exp(-gate))
        scaled = combined * lax.rsqrt(square + EPS) * gain_ref[:, lanes]
        hidden_ref[:, lanes] = (scaled * gate).astype(BF16)
    block = rows // tp
    for piece in range(tp):
        start = pl.multiple_of((quarter ^ piece) * block, block)
        part = hidden_ref[pl.ds(start, block), :]
        pieces[piece][...] = dot(part, w_ref[...]).astype(BF16)


def swap(array, axis, bit):
    size = lax.axis_size(axis)
    return lax.ppermute(array, axis, [(place, place ^ bit) for place in range(size)])


def gather_quarters(own, axis):
    size = lax.axis_size(axis)
    pieces = {0: own}
    bit = size // 2
    while bit:
        for held in list(pieces):
            pieces[held | bit] = swap(pieces[held], axis, bit)
        bit //= 2
    return [pieces[place] for place in range(size)]


def scatter_sum(pieces, axis):
    size = lax.axis_size(axis)
    sums = {place: piece for place, piece in enumerate(pieces)}
    bit = 1
    while bit < size:
        going = [place for place in sums if place & bit]
        arrived = [swap(sums[place].astype(BF16), axis, bit) for place in going]
        for place, piece in zip(going, arrived):
            del sums[place]
            sums[place ^ bit] = sums[place ^ bit].astype(F32) + piece.astype(F32)
        bit *= 2
    return sums[0].astype(BF16)


def routing_kernel(groups, experts, count, me_ref, quarter_ref, rows_hbm, gain_hbm, routes_hbm, *refs):
    outs = refs[:groups]
    rows_ref, gain_ref, routes_ref, sems = refs[groups:]
    slots = 2 * TOPK * count // experts
    per_group = experts * slots // groups
    start = pl.multiple_of(quarter_ref[0] * count, count)
    copies = [
        pltpu.make_async_copy(rows_hbm.at[pl.ds(start, count)], rows_ref, sems.at[0]),
        pltpu.make_async_copy(routes_hbm.at[:, pl.ds(start, count)], routes_ref, sems.at[1]),
        pltpu.make_async_copy(gain_hbm, gain_ref, sems.at[2]),
    ]
    for one in copies:
        one.start()
    for one in copies:
        one.wait()
    wide = rows_ref[...].astype(F32)
    square = jnp.mean(wide * wide, axis=-1, keepdims=True)
    normed = (wide * lax.rsqrt(square + EPS) * gain_ref[...]).astype(BF16)
    row = lax.broadcasted_iota(jnp.int32, (count, count), 0)
    col = lax.broadcasted_iota(jnp.int32, (count, count), 1)
    before = jnp.where(row < col, 1.0, 0.0).astype(BF16)
    expert = lax.broadcasted_iota(jnp.int32, (experts, count), 0)
    member = routes_ref[0:1, :] == expert
    for k in range(1, TOPK):
        member = jnp.logical_or(member, routes_ref[k : k + 1, :] == expert)
    rank = dot(jnp.where(member, 1.0, 0.0).astype(BF16), before)
    rank = jnp.where(member, rank, -1.0).astype(BF16)
    for group, out_ref in enumerate(outs):
        slot = group * per_group + lax.broadcasted_iota(jnp.int32, (per_group, experts), 0)
        which = lax.broadcasted_iota(jnp.int32, (per_group, experts), 1)
        owner = slot // slots
        if groups > 1:
            owner = owner ^ me_ref[0]
        ranks = dot(jnp.where(owner == which, 1.0, 0.0).astype(BF16), rank)
        place = lax.broadcasted_iota(jnp.int32, (per_group, count), 0) % slots
        pick = jnp.where(ranks == place.astype(F32), 1.0, 0.0).astype(BF16)
        out_ref[...] = dot(pick, normed).astype(BF16)


def picks_kernel(groups, experts, me_ref, quarter_ref, routes_ref, factor_ref, pick_ref, weight_ref):
    count = routes_ref.shape[1]
    slots = 2 * TOPK * count // experts
    row = lax.broadcasted_iota(jnp.int32, (count, count), 0)
    col = lax.broadcasted_iota(jnp.int32, (count, count), 1)
    before = jnp.where(row > col, 1.0, 0.0).astype(BF16)

    def column(line):
        return jnp.transpose(jnp.broadcast_to(line, (count, count)))

    named = [column(routes_ref[k : k + 1, :]) for k in range(TOPK)]
    hits = [named[k] == col for k in range(TOPK)]
    member = hits[0]
    for k in range(1, TOPK):
        member = jnp.logical_or(member, hits[k])
    rank = dot(before, jnp.where(member, 1.0, 0.0).astype(BF16))
    slot = lax.broadcasted_iota(jnp.int32, (count, experts * slots), 1)
    for k in range(TOPK):
        place = jnp.sum(jnp.where(hits[k], rank, 0.0), axis=1, keepdims=True).astype(jnp.int32)
        owner = named[k][:, :1]
        if groups > 1:
            owner = owner ^ me_ref[0]
        rows = slice(k * count, (k + 1) * count)
        pick_ref[rows, :] = jnp.where(slot == owner * slots + place, 1.0, 0.0).astype(BF16)
        weight_ref[rows, :] = column(factor_ref[k : k + 1, :])


def hidden_kernel(groups, parts, *refs):
    xs = refs[:groups]
    gates = refs[groups : groups + parts]
    ups = refs[groups + parts : groups + 2 * parts]
    out_ref = refs[-1]
    width = gates[0].shape[1]
    x = jnp.concatenate([one[...] for one in xs], axis=0)
    for i in range(parts):
        gated = dot(x, gates[i][...])
        lifted = dot(x, ups[i][...])
        opened = gated / (1.0 + jnp.exp(-gated))
        out_ref[:, i * width : (i + 1) * width] = (opened * lifted).astype(BF16)


def down_kernel(groups, parts, hidden_ref, *refs):
    downs, outs = refs[:parts], refs[parts:]
    depth, width = downs[0].shape
    rows = hidden_ref.shape[0] // groups
    for first in range(0, width, TILE):
        lanes = slice(first, min(first + TILE, width))
        total = None
        for i in range(parts):
            term = dot(hidden_ref[:, i * depth : (i + 1) * depth], downs[i][:, lanes])
            total = term if total is None else total + term
        result = total.astype(BF16)
        for group, out_ref in enumerate(outs):
            out_ref[:, lanes] = result[group * rows : (group + 1) * rows]


def blend_kernel(groups, pick_ref, weight_ref, *refs):
    arrived = refs[:groups]
    out_ref = refs[-1]
    count = out_ref.shape[0]
    results = jnp.concatenate([one[...] for one in arrived], axis=0)
    chosen = dot(pick_ref[...], results)
    total = None
    for k in range(TOPK):
        rows = slice(k * count, (k + 1) * count)
        term = chosen[rows] * weight_ref[rows, :1]
        total = term if total is None else total + term
    done = 0
    for earlier in refs[groups:-1]:
        out_ref[:, done : done + earlier.shape[1]] = earlier[...]
        done += earlier.shape[1]
    out_ref[:, done : done + total.shape[1]] = total.astype(BF16)


def call(kernel, operands, room=12, **options):
    return pl.pallas_call(kernel, compiler_params=params(room), **options)(*operands)


def shards(
    queries,
    forget_forward_logits,
    forget_backward_logits,
    values,
    output_gate_logits,
    lower_bound_forward,
    lower_bound_backward,
    extra_log_decay,
    head_norm_scale,
    output_projection,
    second_residual,
    expert_norm_scale,
    routes,
    specialist_mixing_factor,
    expert_gate_matrix,
    expert_up_matrix,
    expert_down_matrix,
):
    ep, tp = lax.axis_size("ep"), lax.axis_size("tp")
    direct = ep <= DIRECT_EP
    groups = ep if direct else 1
    me = lax.axis_index("ep").reshape(1).astype(jnp.int32)
    quarter = lax.axis_index("tp").reshape(1).astype(jnp.int32)
    rows_all, model = second_residual.shape
    count = rows_all // tp
    capacity = 2 * TOPK * count
    per_group = capacity // groups
    depth = expert_gate_matrix.shape[2]
    shape = jax.ShapeDtypeStruct
    routes_t = routes.T
    factor_t = specialist_mixing_factor.T

    gates = gather_quarters(expert_gate_matrix[0], "tp")
    ups = gather_quarters(expert_up_matrix[0], "tp")
    edges = [0]
    for share in DOWN_EIGHTHS:
        edges.append(edges[-1] + model * share // sum(DOWN_EIGHTHS))
    parts = list(zip(edges, edges[1:]))
    downs = [gather_quarters(expert_down_matrix[0, :, start:stop], "tp") for start, stop in parts]

    outgoing = call(
        functools.partial(routing_kernel, groups, ep, count),
        (me, quarter, second_residual, expert_norm_scale.reshape(1, -1), routes_t),
        room=60,
        in_specs=[SM, SM, HBM, HBM, HBM],
        out_specs=[VM] * groups,
        out_shape=[shape((per_group, model), BF16)] * groups,
        scratch_shapes=[
            pltpu.VMEM((count, model), BF16),
            pltpu.VMEM((1, model), F32),
            pltpu.VMEM((TOPK, count), routes.dtype),
            pltpu.SemaphoreType.DMA((3,)),
        ],
        cost_estimate=cost(2 * capacity * count * model, 2 * (count + capacity) * model),
    )

    def exchange(blocks):
        if direct:
            return {
                step: swap(block, "ep", step) if step else block
                for step, block in blocks.items()
            }
        stacked = blocks[0].reshape(ep, capacity // ep, -1)
        moved = lax.all_to_all(stacked, "ep", split_axis=0, concat_axis=0, tiled=True)
        return {0: moved.reshape(capacity, -1)}

    arrived = exchange(dict(enumerate(outgoing)))

    rows, key_width = queries.shape
    heads = extra_log_decay.shape[1]
    message = (key_width + TAIL, key_width // heads)
    inner, reach_f, reach_b, total = call(
        functools.partial(recurrence_kernel, heads),
        (
            queries,
            forget_forward_logits,
            forget_backward_logits,
            values,
            lower_bound_forward.reshape(1, -1),
            lower_bound_backward.reshape(1, -1),
            extra_log_decay.T,
        ),
        in_specs=[VM] * 7,
        out_specs=[VM] * 4,
        out_shape=[
            shape((rows, key_width), F32),
            shape((rows, key_width), BF16),
            shape((rows, key_width), BF16),
            shape((2,) + message, BF16),
        ],
        scratch_shapes=[pltpu.VMEM((rows, rows), BF16)],
        cost_estimate=cost(12e9, 8 * rows * key_width, 20 * rows * key_width),
    )
    bit = 1
    before = None
    while bit < ep:
        other = swap(total, "ep", bit)
        if 2 * bit < ep:
            single = 4 * bit >= ep
            total, before = call(
                functools.partial(join_kernel, bit, heads, before is None, single),
                (me, total, other) + (() if before is None else (before,)),
                in_specs=[SM] + [VM] * (2 if before is None else 3),
                out_specs=[VM] * 2,
                out_shape=[
                    shape(message if single else (2,) + message, BF16),
                    shape((2,) + message, F32),
                ],
                cost_estimate=cost(4 * key_width * key_width, 8 * key_width * key_width),
            )
        bit *= 2

    hidden = call(
        functools.partial(hidden_kernel, groups, tp),
        [arrived[step] for step in range(groups)] + gates + ups,
        room=24,
        in_specs=[VM] * (groups + 2 * tp),
        out_specs=VM,
        out_shape=shape((capacity, tp * depth), BF16),
        cost_estimate=cost(4 * capacity * model * tp * depth, 4 * model * tp * depth),
    )
    returned = []
    for i, (start, stop) in enumerate(parts):
        wide = stop - start
        results = call(
            functools.partial(down_kernel, groups, tp),
            [hidden] + downs[i],
            in_specs=[VM] * (1 + tp),
            out_specs=[VM] * groups,
            out_shape=[shape((per_group, wide), BF16)] * groups,
            cost_estimate=cost(2 * capacity * tp * depth * wide, 2 * tp * depth * wide),
        )
        returned.append(exchange(dict(enumerate(results))))

    mixed = call(
        functools.partial(finish_kernel, ep // 2, tp, heads),
        (
            me,
            quarter,
            inner,
            reach_f,
            reach_b,
            output_gate_logits,
            head_norm_scale.reshape(1, -1),
            output_projection,
            other,
            before,
        ),
        in_specs=[SM, SM] + [VM] * 8,
        out_specs=[VM] * tp,
        out_shape=[shape((rows // tp, model), BF16)] * tp,
        scratch_shapes=[pltpu.VMEM((rows, key_width), BF16)],
        cost_estimate=cost(2 * rows * key_width * model, 6 * rows * model, rows * key_width),
    )
    mixer_output = scatter_sum(mixed, "tp")

    def whole(grid_index, a, b):
        return (0, 0)

    pick, weight = call(
        functools.partial(picks_kernel, groups, ep),
        (me, quarter, routes_t, factor_t),
        grid_spec=pltpu.PrefetchScalarGridSpec(
            num_scalar_prefetch=2,
            grid=(1,),
            in_specs=[
                pl.BlockSpec((TOPK, count), lambda i, a, b: (0, b[0])),
                pl.BlockSpec((TOPK, count), whole),
            ],
            out_specs=[
                pl.BlockSpec((TOPK * count, capacity), whole),
                pl.BlockSpec((TOPK * count, count), whole),
            ],
        ),
        out_shape=[shape((TOPK * count, capacity), BF16), shape((TOPK * count, count), F32)],
        cost_estimate=cost(4 * count * count * count, 2 * TOPK * count * capacity),
    )
    ready = []
    for i, (start, stop) in enumerate(parts):
        last = i == len(parts) - 1
        if last:
            pick, mixer_output = lax.optimization_barrier((pick, mixer_output))
        blocks = [returned[i][step] for step in range(groups)]
        ready.append(
            call(
                functools.partial(blend_kernel, groups),
                (pick, weight, *blocks, *(ready if last else [])),
                in_specs=[VM] * (2 + groups + (i if last else 0)),
                out_specs=VM,
                out_shape=shape((count, model if last else stop - start), BF16),
                cost_estimate=cost(
                    2 * TOPK * count * capacity * (stop - start), 2 * capacity * (stop - start)
                ),
            )
        )
    return (mixer_output, ready[-1])


def solution(mesh):
    in_specs = (
        P("ep", "tp"),
        P("ep", "tp"),
        P("ep", "tp"),
        P("ep", "tp"),
        P("ep", "tp"),
        P("tp"),
        P("tp"),
        P("ep", "tp"),
        P("tp"),
        P("tp", None),
        P("ep", None),
        P(),
        P("ep", None),
        P(("ep", "tp"), None),
        P("ep", None, "tp"),
        P("ep", None, "tp"),
        P("ep", "tp", None),
    )
    out_specs = (P(("ep", "tp"), None), P(("ep", "tp"), None))
    return jax.shard_map(shards, mesh=mesh, in_specs=in_specs, out_specs=out_specs, check_vma=False)
```
